512 devices in a mesh: kv: 16 (over y, x), tp: 32 (over z, core).
Axes of the slice: x: 4, y: 4, z: 16, core: 2. Of those that a mesh axis runs over, the one named last changes fastest.
Arguments:
- tokens: bfloat16 [2048, 2048], P('tp', 'kv'), may hold values from -16 to 16
- lengths: int32 [2048], P('tp'), may hold values from 1 to 8192, 2097152 in all
- query_weight: bfloat16 [2048, 1024], P(None, 'kv'), may hold values from -0.125 to 0.125
- key_weight: bfloat16 [2048, 1024], P(None, 'kv'), may hold values from -0.125 to 0.125
- value_weight: bfloat16 [2048, 1024], P(None, 'kv'), may hold values from -0.125 to 0.125
- gate_weight: bfloat16 [2048, 1024], P(None, 'kv'), may hold values from -0.125 to 0.125
- output_weight: bfloat16 [1024, 2048], P('kv'), may hold values from -0.1875 to 0.1875
- mixer_gain: float32 [2048], replicated, may hold values from 0.1 to 1.9
- group_gain: float32 [1024], P('kv'), may hold values from 0.1 to 1.9
- channel_gain: float32 [2048], P('kv'), may hold values from 0.1 to 1.9
- up_weight: bfloat16 [2048, 8192], P('kv', 'tp'), may hold values from -0.125 to 0.125
- down_weight: bfloat16 [8192, 2048], P('tp', 'kv'), may hold values from -0.0625 to 0.0625
- memory_state: float32 [2048, 16, 64, 64], P('tp', 'kv'), may hold values from -0.6 to 0.6
Outputs:
- mixed: bfloat16 [2048, 2048], P('tp', 'kv')
- new_state: float32 [2048, 16, 64, 64], P('tp', 'kv')
The draws below stay inside these ranges and needn't reach their ends.
All inputs are finite; a program needn't handle non-finite values. No bound on the sum of `lengths` on one device may be relied on, other than what follows from the above.
Results may differ from the reference program's by a relative error of at most 0.012.
Values may be sent and summed in bfloat16 or wider, within the bound.
No kernel may reach another device: no remote copies, remote signals or barrier semaphores. Data moves between devices by JAX's collectives and lax.ppermute only.
A program may use at most 64 MiB of HBM per device.

```python
import math
import jax
import jax.numpy as jnp
import numpy as np
from jax import lax

D = 2048
HEADS = 16
HEAD_DIM = 64
FF = 8192
BATCH = 2048
RET_W = 1024


def draw_tokens(key, part):
    noise_key = jax.random.fold_in(key, 11)
    row_key = jax.random.fold_in(key, 12)
    column = jnp.exp(jnp.linspace(jnp.log(0.4), jnp.log(2.4), D)).astype(jnp.float32)
    noise = jax.random.normal(noise_key, (BATCH, D), jnp.float32)
    row_scale = jnp.exp(jax.random.uniform(row_key, (BATCH, 1), jnp.float32, jnp.log(0.5), jnp.log(2.0)))
    values = noise * row_scale * column[None, :]
    return jnp.clip(values, -16.0, 16.0).astype(jnp.bfloat16)


def block_scale(rng, extent, pieces, least, top_value):
    def one(axis_at, parts):
        steps = jax.random.uniform(jax.random.fold_in(jax.random.fold_in(rng, 6), axis_at), (parts,), jnp.float32, least / len(pieces), top_value / len(pieces))
        return jnp.repeat(jnp.exp(steps), extent[axis_at] // parts).reshape((-1,) + (1,) * (len(extent) - axis_at - 1))

    loudness = one(*pieces[0])
    for cut in pieces[1:]:
        loudness = loudness * one(*cut)
    return loudness


def length_profile(number_of, total, bound, slope):
    loads = [(1 << 20) // math.isqrt(grade ** slope) + 1 for grade in range(2, number_of + 1)]
    rest, given = total - bound - (number_of - 1), [1] * (number_of - 1)
    while rest > 0:
        free = [i for i in range(number_of - 1) if given[i] < bound]
        pool, budget = sum([loads[i] for i in free]), rest
        for i in free:
            extra = min(bound - given[i], max(1, budget * loads[i] // pool), rest)
            given[i] = given[i] + extra
            rest = rest - extra
    return np.array([bound] + given)


def uneven_parts(stream_key, number_of, total, most, skew):
    if number_of == 2:
        one = jax.random.randint(stream_key, (), max(1, total - most), min(most, total - 1) + 1)
        return jnp.stack([one, total - one])
    sizes = jnp.asarray(length_profile(number_of, total, most, skew), jnp.int32)
    pairs = (number_of - 1) // 2
    giver, taker = sizes[1:1 + 2 * pairs:2], sizes[2:2 + 2 * pairs:2]
    slack = jnp.minimum(giver - 1, most - taker)
    passed = jax.random.randint(jax.random.fold_in(stream_key, 1), (pairs,), 0, 1 << 20) % (slack + 1)
    sizes = sizes.at[1:1 + 2 * pairs:2].set(giver - passed).at[2:2 + 2 * pairs:2].set(taker + passed)
    return sizes[jax.random.permutation(jax.random.fold_in(stream_key, 2), number_of)]


def bell_draw(rng, shape, scale, limit, split=(), kind=jnp.bfloat16):
    values = scale * jax.random.normal(rng, shape, jnp.float32)
    if split:
        values = values * block_scale(rng, shape, split, -0.22, 0.18)
    return jnp.clip(values, -limit, limit).astype(kind)


def setup_inputs(seed: int = 0) -> dict:
    seeds = jax.random.split(jax.random.key(seed), 14)
    return {
        "tokens": draw_tokens(jax.random.fold_in(seeds[13], 71), 0),
        "lengths": uneven_parts(seeds[1], BATCH, BATCH * 1024, min(8192, BATCH * 256), 2).astype(jnp.int32),
        "query_weight": bell_draw(seeds[2], (D, RET_W), D ** -0.5, 0.125, ((1, 16),)),
        "key_weight": bell_draw(seeds[3], (D, RET_W), D ** -0.5, 0.125, ((1, 16),)),
        "value_weight": bell_draw(seeds[4], (D, RET_W), D ** -0.5, 0.125, ((1, 16),)),
        "gate_weight": bell_draw(seeds[5], (D, RET_W), D ** -0.5, 0.125, ((1, 16),)),
        "output_weight": bell_draw(seeds[6], (RET_W, D), RET_W ** -0.5, 0.1875, ((0, 16),)),
        "mixer_gain": jnp.clip(1.0 + 0.18 * jax.random.normal(seeds[7], (D,), jnp.float32), 0.1, 1.9),
        "group_gain": jnp.clip(1.0 + 0.18 * jax.random.normal(seeds[8], (RET_W,), jnp.float32), 0.1, 1.9),
        "channel_gain": jnp.clip(1.0 + 0.18 * jax.random.normal(seeds[9], (D,), jnp.float32), 0.1, 1.9),
        "up_weight": bell_draw(seeds[10], (D, FF), D ** -0.5, 0.125, ((0, 16), (1, 32))),
        "down_weight": bell_draw(seeds[11], (FF, D), FF ** -0.5, 0.0625, ((0, 32), (1, 16))),
        "memory_state": bell_draw(seeds[12], (BATCH, HEADS, HEAD_DIM, HEAD_DIM), 0.1, 0.6, ((0, 32), (1, 16)), jnp.float32),
    }


EPS = 1e-06
THETA = 10000.0

def rotate(vectors, position):
    breadth = vectors.shape[-1]
    middle = breadth // 2
    inverse = THETA ** (-jnp.arange(middle, dtype=jnp.float32) * 2.0 / breadth)
    angles = position.astype(jnp.float32)[:, None] * inverse[None, :]
    cosine = jnp.cos(angles)[:, None, :]
    sine_part = jnp.sin(angles)[:, None, :]
    former = vectors[..., :middle]
    latter = vectors[..., middle:]
    return jnp.concatenate([former * cosine - latter * sine_part, former * sine_part + latter * cosine], axis=-1)

def reference(tokens, lengths, query_weight, key_weight, value_weight, gate_weight, output_weight, mixer_gain, group_gain, channel_gain, up_weight, down_weight, memory_state):
    served = tokens.shape[0]
    widened = tokens.astype(jnp.float32)
    normed = (widened * lax.rsqrt(lax.optimization_barrier(jnp.mean(widened * widened, axis=1, keepdims=True)) + EPS) * mixer_gain.astype(jnp.float32)).astype(jnp.bfloat16)

    def project(weight):
        return jnp.dot(normed, weight, preferred_element_type=jnp.float32).reshape(served, HEADS, HEAD_DIM)
    queries = rotate(project(query_weight), lengths)
    keys_new = rotate(project(key_weight), lengths) * HEAD_DIM ** (-0.5)
    values_new = project(value_weight)
    gating = jnp.dot(normed, gate_weight, preferred_element_type=jnp.float32)
    head_ids = jnp.arange(HEADS).astype(jnp.float32)
    decays = 1.0 - 2.0 ** (-5.0 - 5.0 * head_ids / (HEADS - 1))
    new_state = decays[None, :, None, None] * memory_state + keys_new[:, :, :, None] * values_new[:, :, None, :]
    readout = jnp.einsum('bhkv,bhk->bhv', new_state, queries, precision=lax.Precision.HIGHEST)
    grouped = readout * lax.rsqrt(lax.optimization_barrier(jnp.mean(readout * readout, axis=-1, keepdims=True)) + EPS)
    grouped = grouped * group_gain.astype(jnp.float32).reshape(HEADS, HEAD_DIM)
    merged = (grouped.reshape(served, HEADS * HEAD_DIM) * jax.nn.silu(gating)).astype(jnp.bfloat16)
    mixed_part = jnp.dot(merged, output_weight, preferred_element_type=jnp.float32)
    after_mixer = (widened + mixed_part).astype(jnp.bfloat16)
    residual = after_mixer.astype(jnp.float32)
    factor = lax.rsqrt(lax.optimization_barrier(jnp.mean(residual * residual, axis=1)) + EPS)
    scaled = (residual * channel_gain.astype(jnp.float32)).astype(jnp.bfloat16)
    raised = jnp.dot(scaled, up_weight, preferred_element_type=jnp.float32) * factor[:, None]
    hidden = jnp.square(jax.nn.relu(raised)).astype(jnp.bfloat16)
    lowered = jnp.dot(hidden, down_weight, preferred_element_type=jnp.float32)
    return ((residual + lowered).astype(jnp.bfloat16), new_state)
```

```python
import jax
import jax.numpy as jnp
import numpy as np
from jax import lax
from jax.sharding import Mesh
from jax.sharding import PartitionSpec as P

D = 2048
HEADS = 16
HEAD_DIM = 64
EPS = 1e-06
THETA = 10000.0

KV = ("y", "xh", "xl")
TP = ("b3", "b2", "b1", "b0", "c")
KAPPA = ("y", "xh")
RHO = ("xl",)
PLANES = ("b1", "b0", "c")
FAR = ("b3", "b2")


def size_of(axes):
    return int(np.prod([lax.axis_size(a) for a in axes]))


def swap(blocks, axes):
    return lax.all_to_all(blocks, axes, split_axis=0, concat_axis=0, tiled=True)


def to_all(value, axes):
    return swap(jnp.broadcast_to(value, (size_of(axes), *value.shape)), axes)


def rotate(vectors, position):
    breadth = vectors.shape[-1]
    middle = breadth // 2
    inverse = THETA ** (-jnp.arange(middle, dtype=jnp.float32) * 2.0 / breadth)
    angles = position.astype(jnp.float32)[:, None] * inverse[None, :]
    cosine = jnp.cos(angles)
    sine = jnp.sin(angles)
    former = vectors[..., :middle]
    latter = vectors[..., middle:]
    return jnp.concatenate(
        [former * cosine - latter * sine, former * sine + latter * cosine], axis=-1
    )


def on_device(
    tokens,
    lengths,
    query_weight,
    key_weight,
    value_weight,
    gate_weight,
    output_weight,
    mixer_gain,
    group_gain,
    channel_gain,
    up_weight,
    down_weight,
    memory_state,
):
    bf16, f32 = jnp.bfloat16, jnp.float32
    served, feats = tokens.shape
    kv, kappa, rho = size_of(KV), size_of(KAPPA), size_of(RHO)
    planes, far = size_of(PLANES), size_of(FAR)
    wide = feats * rho
    units = up_weight.shape[1] // rho

    up_cut = jnp.moveaxis(up_weight.reshape(feats, rho, units), 1, 0)
    down_cut = down_weight.reshape(rho, units, feats)
    first = channel_gain.astype(bf16)
    rest = channel_gain - first.astype(f32)
    second = rest.astype(bf16)
    third = (rest - second.astype(f32)).astype(bf16)
    gain_rows = jnp.concatenate(
        [first[None], second[None], third[None], jnp.zeros((5, feats), bf16)]
    )
    gain_rows = jnp.broadcast_to(gain_rows, (rho, *gain_rows.shape))
    both = jnp.concatenate(
        [up_cut.reshape(rho, -1, 128), down_cut.reshape(rho, -1, 128), gain_rows], axis=1
    )
    both = jnp.broadcast_to(both[:, None], (rho, far, *both.shape[1:]))
    both = swap(both.reshape(rho * far, *both.shape[2:]), RHO + FAR)
    half = (both.shape[1] - 8) // 2
    ups = both[:, :half].reshape(rho, far, feats, units)
    up = jnp.transpose(ups, (0, 2, 1, 3)).reshape(wide, far * units)
    downs = both[:, half : 2 * half].reshape(rho, far, units, feats)
    down = jnp.transpose(downs, (1, 2, 0, 3)).reshape(far * units, wide)
    pieces = both.reshape(rho, far, -1, feats)[:, 0, 2 * half :].astype(f32)
    gains = (pieces[:, 0] + pieces[:, 1] + pieces[:, 2]).reshape(wide)

    blocks = to_all(tokens, KV)
    whole_rows = jnp.moveaxis(blocks, 0, 1).reshape(served, kv * feats)
    widened = whole_rows.astype(f32)
    normed = (
        widened * lax.rsqrt(jnp.mean(widened * widened, axis=1, keepdims=True) + EPS) * mixer_gain
    ).astype(bf16)

    def project(weight):
        return jnp.dot(normed, weight, preferred_element_type=f32)

    queries = rotate(project(query_weight), lengths)
    keys_new = rotate(project(key_weight), lengths) * HEAD_DIM ** (-0.5)
    values_new = project(value_weight)
    gating = project(gate_weight)
    head = lax.axis_index(KV).astype(f32)
    decay = 1.0 - 2.0 ** (-5.0 - 5.0 * head / (HEADS - 1))
    new_state = decay * memory_state[:, 0] + keys_new[:, :, None] * values_new[:, None, :]
    readout = jnp.einsum("bkv,bk->bv", new_state, queries, precision=lax.Precision.HIGHEST)
    grouped = readout * lax.rsqrt(jnp.mean(readout * readout, axis=-1, keepdims=True) + EPS)
    merged = (grouped * group_gain * jax.nn.silu(gating)).astype(bf16)
    shares = jnp.dot(merged, output_weight, preferred_element_type=f32).astype(bf16)

    shares = jnp.moveaxis(shares.reshape(served, kappa, wide), 1, 0)
    shares = jnp.broadcast_to(shares[:, None], (kappa, rho, served, wide)).reshape(kv, served, wide)
    mixed_part = jnp.sum(swap(shares, KV).astype(f32), axis=0)
    at = lax.axis_index(KAPPA) * rho
    own = jnp.moveaxis(lax.dynamic_slice_in_dim(blocks, at, rho, 0), 0, 1).reshape(served, wide)
    after_wide = (own.astype(f32) + mixed_part).astype(bf16)

    rows = to_all(after_wide, PLANES).reshape(planes * served, wide)
    residual = rows.astype(f32)
    squares = jnp.sum(residual * residual, axis=1)
    scaled = (residual * gains).astype(bf16)
    raised_part = jnp.dot(scaled, up, preferred_element_type=f32).astype(bf16)
    part = planes * served // kappa
    hidden_units = far * units
    extra = jnp.zeros((kappa, 8, hidden_units), bf16)
    high = squares.astype(bf16)
    low = (squares - high.astype(f32)).astype(bf16)
    extra = extra.at[:, 0, :part].set(high.reshape(kappa, part))
    extra = extra.at[:, 1, :part].set(low.reshape(kappa, part))
    sent = jnp.concatenate([raised_part.reshape(kappa, part, hidden_units), extra], axis=1)
    arrived = jnp.sum(swap(sent, KAPPA).astype(f32), axis=0)
    raised = arrived[:part]
    totals = arrived[part, :part] + arrived[part + 1, :part]
    factor = lax.rsqrt(totals / D + EPS)
    hidden = jnp.square(jax.nn.relu(raised * factor[:, None])).astype(bf16)
    hidden = to_all(hidden, KAPPA).reshape(planes * served, hidden_units)
    lowered = jnp.dot(hidden, down, preferred_element_type=f32).astype(bf16)

    lowered = lowered.reshape(planes, served, rho, feats)
    lowered = jnp.transpose(lowered, (2, 0, 1, 3)).reshape(rho * planes, served, feats)
    lowered = jnp.sum(swap(lowered, RHO + PLANES).astype(f32), axis=0)
    mine = lax.axis_index(RHO) * feats
    after_mixer = lax.dynamic_slice_in_dim(after_wide, mine, feats, 1)
    mixed = (after_mixer.astype(f32) + lowered).astype(bf16)
    return (mixed, new_state[:, None])


def solution(mesh):
    fine = Mesh(mesh.devices.reshape(4, 2, 2, 2, 2, 2, 2, 2), KV + TP)
    return jax.shard_map(
        on_device,
        mesh=fine,
        in_specs=(
            P(TP, KV),
            P(TP),
            P(None, KV),
            P(None, KV),
            P(None, KV),
            P(None, KV),
            P(KV, None),
            P(None),
            P(KV),
            P(KV),
            P(KV, TP),
            P(TP, KV),
            P(TP, KV, None, None),
        ),
        out_specs=(P(TP, KV), P(TP, KV, None, None)),
        check_vma=False,
    )
```

```python
import jax
import jax.numpy as jnp
import numpy as np
from jax import lax
from jax.sharding import Mesh
from jax.sharding import PartitionSpec as P

D = 2048
HEADS = 16
HEAD_DIM = 64
EPS = 1e-06
THETA = 10000.0

KV = ("y", "xh", "xl")
TP = ("b3", "b2", "b1", "b0", "c")
KAPPA = ("y", "xh")
RHO = ("xl",)
PLANES = ("b1", "b0", "c")
FAR = ("b3", "b2")


def size_of(axes):
    return int(np.prod([lax.axis_size(a) for a in axes]))


def swap(blocks, axes):
    return lax.all_to_all(blocks, axes, split_axis=0, concat_axis=0, tiled=True)


def to_all(value, axes):
    return swap(jnp.broadcast_to(value, (size_of(axes), *value.shape)), axes)


def rotate(vectors, position):
    breadth = vectors.shape[-1]
    middle = breadth // 2
    inverse = THETA ** (-jnp.arange(middle, dtype=jnp.float32) * 2.0 / breadth)
    angles = position.astype(jnp.float32)[:, None] * inverse[None, :]
    cosine = jnp.cos(angles)
    sine = jnp.sin(angles)
    former = vectors[..., :middle]
    latter = vectors[..., middle:]
    return jnp.concatenate(
        [former * cosine - latter * sine, former * sine + latter * cosine], axis=-1
    )


def layer(
    tokens,
    lengths,
    query_weight,
    key_weight,
    value_weight,
    gate_weight,
    output_weight,
    mixer_gain,
    group_gain,
    channel_gain,
    up_weight,
    down_weight,
    memory_state,
):
    bf16, f32 = jnp.bfloat16, jnp.float32
    served, feats = tokens.shape
    kv, kappa, rho = size_of(KV), size_of(KAPPA), size_of(RHO)
    planes, far = size_of(PLANES), size_of(FAR)
    wide = feats * rho
    units = up_weight.shape[1] // rho

    up_cut = jnp.moveaxis(up_weight.reshape(feats, rho, units), 1, 0)
    down_cut = down_weight.reshape(rho, units, feats)
    first = channel_gain.astype(bf16)
    rest = channel_gain - first.astype(f32)
    second = rest.astype(bf16)
    third = (rest - second.astype(f32)).astype(bf16)
    gain_rows = jnp.concatenate(
        [first[None], second[None], third[None], jnp.zeros((5, feats), bf16)]
    )
    gain_rows = jnp.broadcast_to(gain_rows, (rho, *gain_rows.shape))
    both = jnp.concatenate(
        [up_cut.reshape(rho, -1, 128), down_cut.reshape(rho, -1, 128), gain_rows], axis=1
    )
    side = lax.axis_index(RHO)
    got = lax.ppermute(both[1 - side], RHO, [(0, 1), (1, 0)])
    pair = jnp.where(side == 0, jnp.stack([both[0], got]), jnp.stack([got, both[1]]))
    pairs = [pair]
    for step in (2, 1, 3):
        pairs.append(lax.ppermute(pair, FAR, [(i, (i + step) % far) for i in range(far)]))
    half = (pair.shape[1] - 8) // 2
    up = jnp.concatenate([p[:, :half].reshape(wide, units) for p in pairs], axis=1)
    down = jnp.concatenate(
        [jnp.moveaxis(p[:, half : 2 * half], 0, 1).reshape(units, wide) for p in pairs]
    )
    pieces = pair[:, 2 * half :].astype(f32)
    gains = (pieces[:, 0] + pieces[:, 1] + pieces[:, 2]).reshape(wide)

    blocks = to_all(tokens, KV)
    whole_rows = jnp.moveaxis(blocks, 0, 1).reshape(served, kv * feats)
    widened = whole_rows.astype(f32)
    normed = (
        widened * lax.rsqrt(jnp.mean(widened * widened, axis=1, keepdims=True) + EPS) * mixer_gain
    ).astype(bf16)

    def project(weight):
        return jnp.dot(normed, weight, preferred_element_type=f32)

    queries = rotate(project(query_weight), lengths)
    keys_new = rotate(project(key_weight), lengths) * HEAD_DIM ** (-0.5)
    values_new = project(value_weight)
    gating = project(gate_weight)
    head = lax.axis_index(KV).astype(f32)
    decay = 1.0 - 2.0 ** (-5.0 - 5.0 * head / (HEADS - 1))
    new_state = decay * memory_state[:, 0] + keys_new[:, :, None] * values_new[:, None, :]
    readout = jnp.einsum("bkv,bk->bv", new_state, queries, precision=lax.Precision.HIGHEST)
    grouped = readout * lax.rsqrt(jnp.mean(readout * readout, axis=-1, keepdims=True) + EPS)
    merged = (grouped * group_gain * jax.nn.silu(gating)).astype(bf16)
    shares = jnp.dot(merged, output_weight, preferred_element_type=f32).astype(bf16)

    shares = jnp.moveaxis(shares.reshape(served, kappa, wide), 1, 0)
    shares = jnp.broadcast_to(shares[:, None], (kappa, rho, served, wide)).reshape(kv, served, wide)
    shares = swap(shares, KV)
    mixed_part = jnp.sum(shares.astype(f32), axis=0)
    at = lax.axis_index(KAPPA) * rho
    own = jnp.moveaxis(lax.dynamic_slice_in_dim(blocks, at, rho, 0), 0, 1).reshape(served, wide)
    after_wide = (own.astype(f32) + mixed_part).astype(bf16)

    rows = to_all(after_wide, PLANES).reshape(planes * served, wide)
    residual = rows.astype(f32)
    squares = jnp.sum(residual * residual, axis=1)
    scaled = (residual * gains).astype(bf16)
    raised_part = jnp.dot(scaled, up, preferred_element_type=f32).astype(bf16)
    part = planes * served // kappa
    hidden_units = far * units
    extra = jnp.zeros((kappa, 8, hidden_units), bf16)
    high = squares.astype(bf16)
    low = (squares - high.astype(f32)).astype(bf16)
    extra = extra.at[:, 0, :part].set(high.reshape(kappa, part))
    extra = extra.at[:, 1, :part].set(low.reshape(kappa, part))
    sent = jnp.concatenate([raised_part.reshape(kappa, part, hidden_units), extra], axis=1)
    arrived = jnp.sum(swap(sent, KAPPA).astype(f32), axis=0)
    raised = arrived[:part]
    totals = arrived[part, :part] + arrived[part + 1, :part]
    factor = lax.rsqrt(totals / D + EPS)
    hidden = jnp.square(jax.nn.relu(raised * factor[:, None])).astype(bf16)
    hidden = to_all(hidden, KAPPA).reshape(planes * served, hidden_units)
    lowered = jnp.dot(hidden, down, preferred_element_type=f32).astype(bf16)

    lowered = lowered.reshape(planes, served, rho, feats)
    lowered = jnp.transpose(lowered, (2, 0, 1, 3)).reshape(rho * planes, served, feats)
    lowered = jnp.sum(swap(lowered, RHO + PLANES).astype(f32), axis=0)
    mine = lax.axis_index(RHO) * feats
    after_mixer = lax.dynamic_slice_in_dim(after_wide, mine, feats, 1)
    mixed = (after_mixer.astype(f32) + lowered).astype(bf16)
    return (mixed, new_state[:, None])


def solution(mesh):
    fine = Mesh(mesh.devices.reshape(4, 2, 2, 2, 2, 2, 2, 2), KV + TP)
    return jax.shard_map(
        layer,
        mesh=fine,
        in_specs=(
            P(TP, KV),
            P(TP),
            P(None, KV),
            P(None, KV),
            P(None, KV),
            P(None, KV),
            P(KV, None),
            P(None),
            P(KV),
            P(KV),
            P(KV, TP),
            P(TP, KV),
            P(TP, KV, None, None),
        ),
        out_specs=(P(TP, KV), P(TP, KV, None, None)),
        check_vma=False,
    )
```

```python
import jax
import jax.numpy as jnp
import numpy as np
from jax import lax
from jax.experimental import pallas as pl
from jax.experimental.pallas import tpu as pltpu
from jax.sharding import Mesh
from jax.sharding import PartitionSpec as P

D = 2048
HEADS = 16
HEAD_DIM = 64
EPS = 1e-06
THETA = 10000.0

KV = ("y", "xh", "xl")
TP = ("b3", "b2", "b1", "b0", "c")
KAPPA = ("y", "xh")
RHO = ("xl",)
PLANES = ("b1", "b0", "c")
FAR = ("b3", "b2")


def size_of(axes):
    return int(np.prod([lax.axis_size(a) for a in axes]))


def swap(blocks, axes):
    return lax.all_to_all(blocks, axes, split_axis=0, concat_axis=0, tiled=True)


def to_all(value, axes):
    return swap(jnp.broadcast_to(value, (size_of(axes), *value.shape)), axes)


def rotate(vectors, position):
    breadth = vectors.shape[-1]
    middle = breadth // 2
    inverse = THETA ** (-jnp.arange(middle, dtype=jnp.float32) * 2.0 / breadth)
    angles = position.astype(jnp.float32)[:, None] * inverse[None, :]
    cosine = jnp.cos(angles)
    sine = jnp.sin(angles)
    former = vectors[..., :middle]
    latter = vectors[..., middle:]
    return jnp.concatenate(
        [former * cosine - latter * sine, former * sine + latter * cosine], axis=-1
    )


def call(kernel, out, *operands, scalars=(), flops=1 << 20):
    moved = sum(o.size * o.dtype.itemsize for o in operands)
    moved += int(np.prod(out.shape)) * out.dtype.itemsize
    smem = pl.BlockSpec(memory_space=pltpu.SMEM)
    vmem = pl.BlockSpec(memory_space=pltpu.VMEM)
    return pl.pallas_call(
        kernel,
        out_shape=out,
        in_specs=[smem] * len(scalars) + [vmem] * len(operands),
        out_specs=vmem,
        compiler_params=pltpu.CompilerParams(vmem_limit_bytes=24 << 20),
        cost_estimate=pl.CostEstimate(flops=flops, bytes_accessed=moved, transcendentals=0),
    )(*(jnp.reshape(v, (1,)).astype(jnp.int32) for v in scalars), *operands)


def pack_kernel(up_ref, down_ref, gain_ref, out_ref):
    bf16, f32 = jnp.bfloat16, jnp.float32
    feats, units = up_ref.shape[0], up_ref.shape[1] // out_ref.shape[0]
    gain = gain_ref[...]
    first = gain.astype(bf16).astype(f32)
    second = (gain - first).astype(bf16).astype(f32)
    third = gain - first - second
    row = lax.broadcasted_iota(jnp.int32, (8, feats), 0)
    zero = jnp.zeros((8, feats), f32)
    rows = jnp.where(row == 0, first, jnp.where(row == 1, second, jnp.where(row == 2, third, zero)))
    for r in range(out_ref.shape[0]):
        out_ref[r, :feats] = up_ref[:, r * units : (r + 1) * units]
        out_ref[r, feats : feats + units] = down_ref[r * units : (r + 1) * units]
        out_ref[r, feats + units :] = rows.astype(bf16)


def pick_kernel(side_ref, *refs):
    *blocks, out_ref = refs
    for d, block in enumerate(blocks):
        out_ref[d] = block[1 - side_ref[0]]


def after_kernel(at_ref, parts_ref, tokens_ref, out_ref):
    f32 = jnp.float32
    feats = tokens_ref.shape[2]
    total = parts_ref[0].astype(f32)
    for k in range(1, parts_ref.shape[0]):
        total = total + parts_ref[k].astype(f32)
    rho = out_ref.shape[2] // feats
    for r in range(rho):
        own = tokens_ref[at_ref[0] + r].astype(f32)
        block = (own + total[:, r * feats : (r + 1) * feats]).astype(jnp.bfloat16)
        for p in range(out_ref.shape[0]):
            out_ref[p, :, r * feats : (r + 1) * feats] = block


def up_kernel(side_ref, rows_ref, got_ref, *refs):
    bf16, f32 = jnp.bfloat16, jnp.float32
    *blocks, out_ref = refs
    planes, served, wide = rows_ref.shape
    kappa, _, _ = out_ref.shape
    feats = wide // 2
    count = planes * served
    side = side_ref[0]
    rows = rows_ref[...].reshape(count, wide)
    x = rows.astype(f32)
    kept = jnp.where(side == 0, x[:, :feats], x[:, feats:])
    other = jnp.where(side == 0, x[:, feats:], x[:, :feats])
    bottom = blocks[0].shape[1] - 8

    def gain_of(pieces):
        p = pieces.astype(f32)
        return p[0:1] + p[1:2] + p[2:3]

    mine = blocks[0][side]
    kept = (kept * gain_of(mine[bottom:])).astype(bf16)
    other = (other * gain_of(got_ref[0, bottom:])).astype(bf16)
    for d, block in enumerate(blocks):
        part = jnp.dot(kept, block[side, :feats], preferred_element_type=f32)
        part = part + jnp.dot(other, got_ref[d, :feats], preferred_element_type=f32)
        units = part.shape[1]
        part = part.astype(bf16).reshape(kappa, count // kappa, units)
        out_ref[:, : count // kappa, d * units : (d + 1) * units] = part
    square = x * x
    high = square.astype(bf16)
    low = (square - high.astype(f32)).astype(bf16)
    ones = jnp.ones((8, wide), bf16)
    along = (((1,), (1,)), ((), ()))
    total = lax.dot_general(ones, high, along, preferred_element_type=f32)
    total = total + lax.dot_general(ones, low, along, preferred_element_type=f32)
    high = total.astype(bf16).astype(f32)
    low = total - high
    row = lax.broadcasted_iota(jnp.int32, total.shape, 0)
    extra = jnp.where(row == 0, high, jnp.where(row == 1, low, jnp.zeros_like(total))).astype(bf16)
    for k in range(kappa):
        out_ref[k, count // kappa :] = extra


def hidden_kernel(at_ref, parts_ref, out_ref):
    f32 = jnp.float32
    count = out_ref.shape[1]
    total = parts_ref[0].astype(f32)
    for k in range(1, parts_ref.shape[0]):
        total = total + parts_ref[k].astype(f32)
    squares = total[count : count + 1] + total[count + 1 : count + 2]
    shape = (count, total.shape[1])
    row = lax.broadcasted_iota(jnp.int32, shape, 0)
    lane = lax.broadcasted_iota(jnp.int32, shape, 1)
    mine = jnp.where(lane == row + at_ref[0] * count, squares, jnp.zeros(shape, f32))
    factor = lax.rsqrt(jnp.sum(mine, axis=1, keepdims=True) / D + EPS)
    raised = jnp.maximum(total[:count] * factor, 0.0)
    hidden = (raised * raised).astype(jnp.bfloat16)
    for k in range(out_ref.shape[0]):
        out_ref[k] = hidden


def down_kernel(side_ref, hidden_ref, got_ref, *refs):
    *blocks, out_ref = refs
    kappa, rows, units = hidden_ref.shape
    _, planes, served, feats = out_ref.shape
    start = feats
    stop = blocks[0].shape[1] - 8
    side = side_ref[0]
    hidden = hidden_ref[...].reshape(kappa * rows, units)
    kept = jnp.concatenate([b[side, start:stop] for b in blocks])
    other = jnp.concatenate([got_ref[d, start:stop] for d in range(len(blocks))])
    for at, weight in ((side, kept), (1 - side, other)):
        part = jnp.dot(hidden, weight, preferred_element_type=jnp.float32)
        out_ref[at] = part.astype(jnp.bfloat16).reshape(planes, served, feats)


def final_kernel(side_ref, parts_ref, after_ref, out_ref):
    f32 = jnp.float32
    feats = out_ref.shape[1]
    total = parts_ref[0].astype(f32)
    for k in range(1, parts_ref.shape[0]):
        total = total + parts_ref[k].astype(f32)
    after = after_ref[0].astype(f32)
    after = jnp.where(side_ref[0] == 0, after[:, :feats], after[:, feats:])
    out_ref[...] = (after + total).astype(out_ref.dtype)


def layer(
    tokens,
    lengths,
    query_weight,
    key_weight,
    value_weight,
    gate_weight,
    output_weight,
    mixer_gain,
    group_gain,
    channel_gain,
    up_weight,
    down_weight,
    memory_state,
):
    bf16, f32 = jnp.bfloat16, jnp.float32
    served, feats = tokens.shape
    kv, kappa, rho = size_of(KV), size_of(KAPPA), size_of(RHO)
    planes, far = size_of(PLANES), size_of(FAR)
    wide = feats * rho
    units = up_weight.shape[1] // rho

    like = jax.ShapeDtypeStruct
    both = call(
        pack_kernel,
        like((rho, feats + units + 8, feats), bf16),
        up_weight,
        down_weight,
        channel_gain.reshape(1, feats),
    )
    blocks_far = [both]
    for step in (2, 1, 3):
        ring = [(i, (i + step) % far) for i in range(far)]
        blocks_far.append(lax.ppermute(both, FAR, ring))
    side = lax.axis_index(RHO)
    given = call(
        pick_kernel, like((far, *both.shape[1:]), bf16), *blocks_far, scalars=(side,)
    )
    got = lax.ppermute(given, RHO, [(0, 1), (1, 0)])

    blocks = to_all(tokens, KV)
    whole_rows = jnp.moveaxis(blocks, 0, 1).reshape(served, kv * feats)
    widened = whole_rows.astype(f32)
    normed = (
        widened * lax.rsqrt(jnp.mean(widened * widened, axis=1, keepdims=True) + EPS) * mixer_gain
    ).astype(bf16)

    def project(weight):
        return jnp.dot(normed, weight, preferred_element_type=f32)

    queries = rotate(project(query_weight), lengths)
    keys_new = rotate(project(key_weight), lengths) * HEAD_DIM ** (-0.5)
    values_new = project(value_weight)
    gating = project(gate_weight)
    head = lax.axis_index(KV).astype(f32)
    decay = 1.0 - 2.0 ** (-5.0 - 5.0 * head / (HEADS - 1))
    new_state = decay * memory_state[:, 0] + keys_new[:, :, None] * values_new[:, None, :]
    readout = jnp.einsum("bkv,bk->bv", new_state, queries, precision=lax.Precision.HIGHEST)
    grouped = readout * lax.rsqrt(jnp.mean(readout * readout, axis=-1, keepdims=True) + EPS)
    merged = (grouped * group_gain * jax.nn.silu(gating)).astype(bf16)
    shares = jnp.dot(merged, output_weight, preferred_element_type=f32).astype(bf16)

    shares = jnp.moveaxis(shares.reshape(served, kappa, wide), 1, 0)
    shares = jnp.broadcast_to(shares[:, None], (kappa, rho, served, wide)).reshape(kv, served, wide)
    shares = swap(shares, KV)
    at = lax.axis_index(KAPPA) * rho
    after_wide = call(
        after_kernel, like((planes, served, wide), bf16), shares, blocks, scalars=(at,)
    )

    rows = swap(after_wide, PLANES)
    part = planes * served // kappa
    sent = call(
        up_kernel,
        like((kappa, part + 8, far * units), bf16),
        rows,
        got,
        *blocks_far,
        scalars=(side,),
        flops=2 * planes * served * wide * far * units,
    )
    hidden = call(
        hidden_kernel,
        like((kappa, part, far * units), bf16),
        swap(sent, KAPPA),
        scalars=(lax.axis_index(KAPPA),),
    )
    lowered = call(
        down_kernel,
        like((rho, planes, served, feats), bf16),
        swap(hidden, KAPPA),
        got,
        *blocks_far,
        scalars=(side,),
        flops=2 * planes * served * wide * far * units,
    )

    lowered = swap(lowered.reshape(rho * planes, served, feats), RHO + PLANES)
    mixed = call(final_kernel, like((served, feats), bf16), lowered, after_wide, scalars=(side,))
    return (mixed, new_state[:, None])


def solution(mesh):
    fine = Mesh(mesh.devices.reshape(4, 2, 2, 2, 2, 2, 2, 2), KV + TP)
    return jax.shard_map(
        layer,
        mesh=fine,
        in_specs=(
            P(TP, KV),
            P(TP),
            P(None, KV),
            P(None, KV),
            P(None, KV),
            P(None, KV),
            P(KV, None),
            P(None),
            P(KV),
            P(KV),
            P(KV, TP),
            P(TP, KV),
            P(TP, KV, None, None),
        ),
        out_specs=(P(TP, KV), P(TP, KV, None, None)),
        check_vma=False,
    )
```

```python
import jax
import jax.numpy as jnp
import numpy as np
from jax import lax
from jax.experimental import pallas as pl
from jax.experimental.pallas import tpu as pltpu
from jax.sharding import Mesh
from jax.sharding import PartitionSpec as P

D = 2048
HEADS = 16
HEAD_DIM = 64
EPS = 1e-06
THETA = 10000.0

KV = ("y", "xh", "xl")
TP = ("b3", "b2", "b1", "b0", "c")
HALF = "xl"
COLS = ("y", "xh")
PLANES = ("b0", "c")
FAR = ("b3", "b2", "b1")

bf16, f32 = jnp.bfloat16, jnp.float32
NT = (((1,), (1,)), ((), ()))


def size_of(axes):
    return int(np.prod([lax.axis_size(a) for a in axes]))


def swap(blocks, axes):
    return lax.all_to_all(blocks, axes, split_axis=0, concat_axis=0, tiled=True)


def call(kernel, out, *operands, scalars=(), flops=1 << 20):
    outs = out if isinstance(out, tuple) else (out,)
    moved = sum(o.size * o.dtype.itemsize for o in operands)
    moved += sum(int(np.prod(o.shape)) * o.dtype.itemsize for o in outs)
    smem = pl.BlockSpec(memory_space=pltpu.SMEM)
    vmem = pl.BlockSpec(memory_space=pltpu.VMEM)
    return pl.pallas_call(
        kernel,
        out_shape=out,
        in_specs=[smem] * len(scalars) + [vmem] * len(operands),
        out_specs=(vmem,) * len(out) if isinstance(out, tuple) else vmem,
        compiler_params=pltpu.CompilerParams(vmem_limit_bytes=32 << 20),
        cost_estimate=pl.CostEstimate(flops=flops, bytes_accessed=moved, transcendentals=0),
    )(*(jnp.reshape(v, (1,)) for v in scalars), *operands)


def pack_kernel(tokens_ref, up_ref, down_ref, gain_ref, out_ref):
    served, feats = tokens_ref.shape
    cols = out_ref.shape[0] // 2
    units = up_ref.shape[1] // cols
    gain = gain_ref[...]
    first = gain.astype(bf16).astype(f32)
    second = (gain - first).astype(bf16).astype(f32)
    third = gain - first - second
    row = lax.broadcasted_iota(jnp.int32, (8, feats), 0)
    zero = jnp.zeros((8, feats), f32)
    rows = jnp.where(row == 0, first, jnp.where(row == 1, second, jnp.where(row == 2, third, zero)))
    rows = rows.astype(bf16)
    up = up_ref[...].astype(f32).T.astype(bf16)
    tokens = tokens_ref[...]
    at = served + 2 * units
    for j in range(cols):
        for half in range(2):
            k = 2 * j + half
            out_ref[k, :served] = tokens
            out_ref[k, served : served + units] = up[j * units : (j + 1) * units]
            out_ref[k, served + units : at] = down_ref[j * units : (j + 1) * units]
            out_ref[k, at:] = rows


def unpack_kernel(side_ref, arrived_ref, gain_ref, mine_ref, normed_ref):
    feats = arrived_ref.shape[2]
    served = normed_ref.shape[0]
    both = mine_ref.shape[0]
    for j in range(arrived_ref.shape[0] // 2):
        mine_ref[:, j * feats : (j + 1) * feats] = arrived_ref[
            2 * j + side_ref[0], served : served + both
        ]
    total = jnp.zeros((served, feats), f32)
    for k in range(arrived_ref.shape[0]):
        x = arrived_ref[k, :served].astype(f32)
        total = total + x * x
    factor = lax.rsqrt(jnp.sum(total, axis=1, keepdims=True) / D + EPS)
    for k in range(arrived_ref.shape[0]):
        at = slice(k * feats, (k + 1) * feats)
        x = arrived_ref[k, :served].astype(f32)
        normed_ref[:, at] = (x * factor * gain_ref[:, at]).astype(bf16)


def retention_kernel(
    decay_ref,
    normed_ref,
    query_ref,
    key_ref,
    value_ref,
    gate_ref,
    output_ref,
    cosine_ref,
    sine_ref,
    state_ref,
    gain_ref,
    shares_ref,
    keys_ref,
    values_ref,
    readout_ref,
):
    normed = normed_ref[...]
    middle = HEAD_DIM // 2

    def project(weight):
        return lax.dot_general(normed, weight, NT, preferred_element_type=f32)

    def rotated(ref):
        plain = project(ref[...])
        turned = project(jnp.concatenate([ref[middle:], ref[:middle]]))
        return plain * cosine_ref[...] + turned * sine_ref[...]

    queries = rotated(query_ref)
    keys = rotated(key_ref) * HEAD_DIM ** (-0.5)
    values = project(value_ref[...])
    gating = project(gate_ref[...])
    keys_ref[...] = keys
    values_ref[...] = values
    columns = queries.T
    for b in range(state_ref.shape[0]):
        readout_ref[b : b + 1] = jnp.sum(state_ref[b] * columns[:, b : b + 1], axis=0, keepdims=True)
    matched = jnp.sum(keys * queries, axis=1, keepdims=True)
    readout = decay_ref[0] * readout_ref[...] + matched * values
    square = jnp.sum(readout * readout, axis=1, keepdims=True) / HEAD_DIM
    grouped = readout * lax.rsqrt(square + EPS) * gain_ref[...]
    merged = (grouped * (gating * jax.nn.sigmoid(gating))).astype(bf16)
    shares = jnp.dot(merged, output_ref[...], preferred_element_type=f32).astype(bf16)
    feats = shares_ref.shape[2]
    for k in range(shares_ref.shape[0]):
        shares_ref[k] = shares[:, k * feats : (k + 1) * feats]


def sum_of(parts_ref):
    total = parts_ref[0].astype(f32)
    for k in range(1, parts_ref.shape[0]):
        total = total + parts_ref[k].astype(f32)
    return total


def after_kernel(parts_ref, tokens_ref, out_ref):
    block = (tokens_ref[...].astype(f32) + sum_of(parts_ref)).astype(bf16)
    for p in range(out_ref.shape[0]):
        out_ref[p] = block


def up_kernel(side_ref, rows_ref, arrived_ref, weights_ref, own_ref, sent_ref):
    cols, count, feats = rows_ref.shape
    lines = arrived_ref.shape[1]
    far = weights_ref.shape[0] // 64
    units = weights_ref.shape[0] // (2 * far)
    ones = jnp.ones((8, feats), bf16)
    total = jnp.zeros((8, count), f32)
    scaled = []
    for j in range(cols):
        x = rows_ref[j].astype(f32)
        pieces = arrived_ref[2 * j + side_ref[0], lines - 8 :].astype(f32)
        scaled.append((x * (pieces[0:1] + pieces[1:2] + pieces[2:3])).astype(bf16))
        square = x * x
        high = square.astype(bf16)
        low = (square - high.astype(f32)).astype(bf16)
        total = total + lax.dot_general(ones, high, NT, preferred_element_type=f32)
        total = total + lax.dot_general(ones, low, NT, preferred_element_type=f32)
    weight = jnp.concatenate(
        [weights_ref[2 * f * units : (2 * f + 1) * units] for f in range(far)]
    )
    part = lax.dot_general(
        jnp.concatenate(scaled, axis=1), weight, NT, preferred_element_type=f32
    )
    own_ref[:count] = part
    sent_ref[:count] = part.astype(bf16)
    high = total.astype(bf16).astype(f32)
    low = total - high
    row = lax.broadcasted_iota(jnp.int32, total.shape, 0)
    extra = jnp.where(row == 0, high, jnp.where(row == 1, low, jnp.zeros_like(total)))
    own_ref[count:] = extra
    sent_ref[count:] = extra.astype(bf16)


def down_kernel(own_ref, other_ref, weights_ref, out_ref):
    cols, count, feats = out_ref.shape
    far = weights_ref.shape[0] // 64
    units = weights_ref.shape[0] // (2 * far)
    total = own_ref[...] + other_ref[...].astype(f32)
    squares = total[count : count + 1] + total[count + 1 : count + 2]
    row = lax.broadcasted_iota(jnp.int32, (count, count), 0)
    lane = lax.broadcasted_iota(jnp.int32, (count, count), 1)
    mine = jnp.where(lane == row, squares, jnp.zeros((count, count), f32))
    factor = lax.rsqrt(jnp.sum(mine, axis=1, keepdims=True) / D + EPS)
    raised = jnp.maximum(total[:count] * factor, 0.0)
    hidden = (raised * raised).astype(bf16)
    weight = jnp.concatenate(
        [weights_ref[(2 * f + 1) * units : (2 * f + 2) * units] for f in range(far)]
    )
    part = jnp.dot(hidden, weight, preferred_element_type=f32).astype(bf16)
    for j in range(cols):
        out_ref[j] = part[:, j * feats : (j + 1) * feats]


def final_kernel(parts_ref, after_ref, out_ref):
    out_ref[...] = (after_ref[0].astype(f32) + sum_of(parts_ref)).astype(out_ref.dtype)


def layer(
    tokens,
    lengths,
    query_weight,
    key_weight,
    value_weight,
    gate_weight,
    output_weight,
    mixer_gain,
    group_gain,
    channel_gain,
    up_weight,
    down_weight,
    memory_state,
):
    like = jax.ShapeDtypeStruct
    served, feats = tokens.shape
    kv, cols, planes, far = size_of(KV), size_of(COLS), size_of(PLANES), size_of(FAR)
    units = up_weight.shape[1] // cols
    count = planes * served
    side = lax.axis_index(HALF)

    sent = call(
        pack_kernel,
        like((kv, served + 2 * units + 8, feats), bf16),
        tokens,
        up_weight,
        down_weight,
        channel_gain.reshape(1, feats),
    )
    arrived = swap(sent, KV)
    mine, normed = call(
        unpack_kernel,
        (like((2 * units, cols * feats), bf16), like((served, kv * feats), bf16)),
        arrived,
        mixer_gain.reshape(1, kv * feats),
        scalars=(side,),
    )
    weights = lax.all_gather(mine, FAR, axis=0, tiled=True)

    middle = HEAD_DIM // 2
    inverse = THETA ** (-jnp.arange(middle, dtype=f32) * 2.0 / HEAD_DIM)
    angles = lengths.astype(f32)[:, None] * inverse[None, :]
    cosine, sine = jnp.cos(angles), jnp.sin(angles)
    head = lax.axis_index(KV).astype(f32)
    decay = 1.0 - 2.0 ** (-5.0 - 5.0 * head / (HEADS - 1))
    state = memory_state[:, 0]
    shares, keys_new, values_new, _ = call(
        retention_kernel,
        (
            like((kv, served, feats), bf16),
            like((served, HEAD_DIM), f32),
            like((served, HEAD_DIM), f32),
            like((served, HEAD_DIM), f32),
        ),
        normed,
        query_weight.T,
        key_weight.T,
        value_weight.T,
        gate_weight.T,
        output_weight,
        jnp.concatenate([cosine, cosine], axis=1),
        jnp.concatenate([-sine, sine], axis=1),
        state,
        group_gain.reshape(1, HEAD_DIM),
        scalars=(decay,),
        flops=2 * served * D * 6 * HEAD_DIM,
    )
    shares = swap(shares, KV)
    after = call(after_kernel, like((cols * planes, served, feats), bf16), shares, tokens)

    rows = swap(after, COLS + PLANES).reshape(cols, count, feats)
    own, given = call(
        up_kernel,
        (like((count + 8, far * units), f32), like((count + 8, far * units), bf16)),
        rows,
        arrived,
        weights,
        scalars=(side,),
        flops=2 * count * cols * feats * far * units,
    )
    other = lax.ppermute(given, HALF, [(0, 1), (1, 0)])
    lowered = call(
        down_kernel,
        like((cols, count, feats), bf16),
        own,
        other,
        weights,
        flops=2 * count * cols * feats * far * units,
    )

    lowered = swap(lowered.reshape(cols * planes, served, feats), COLS + PLANES)
    mixed = call(final_kernel, like((served, feats), bf16), lowered, after)
    new_state = decay * state + keys_new[:, :, None] * values_new[:, None, :]
    return (mixed, new_state[:, None])


def solution(mesh):
    fine = Mesh(mesh.devices.reshape(4, 2, 2, 2, 2, 2, 2, 2), KV + TP)
    return jax.shard_map(
        layer,
        mesh=fine,
        in_specs=(
            P(TP, KV),
            P(TP),
            P(None, KV),
            P(None, KV),
            P(None, KV),
            P(None, KV),
            P(KV, None),
            P(None),
            P(KV),
            P(KV),
            P(KV, TP),
            P(TP, KV),
            P(TP, KV, None, None),
        ),
        out_specs=(P(TP, KV), P(TP, KV, None, None)),
        check_vma=False,
    )
```

```python
import jax
import jax.numpy as jnp
import numpy as np
from jax import lax
from jax.experimental import pallas as pl
from jax.experimental.pallas import tpu as pltpu
from jax.sharding import Mesh
from jax.sharding import PartitionSpec as P

D = 2048
HEADS = 16
HEAD_DIM = 64
EPS = 1e-06
THETA = 10000.0

KV = ("y", "xh", "xl")
TP = ("b3", "b2", "b1", "b0", "c")
HALF = "xl"
COLS = ("y", "xh")
PLANES = ("b0", "c")
FAR = ("b3", "b2", "b1")

bf16, f32 = jnp.bfloat16, jnp.float32
NT = (((1,), (1,)), ((), ()))


def size_of(axes):
    return int(np.prod([lax.axis_size(a) for a in axes]))


def swap(blocks, axes):
    return lax.all_to_all(blocks, axes, split_axis=0, concat_axis=0, tiled=True)


def call(kernel, out, *operands, scalars=(), hbm=(), scratch=(), limit=16 << 20, flops=1 << 20):
    outs = out if isinstance(out, tuple) else (out,)
    moved = sum(o.size * o.dtype.itemsize for o in operands)
    moved += sum(int(np.prod(o.shape)) * o.dtype.itemsize for o in outs)
    smem = pl.BlockSpec(memory_space=pltpu.SMEM)
    vmem = pl.BlockSpec(memory_space=pltpu.VMEM)
    far = pl.BlockSpec(memory_space=pltpu.HBM)
    return pl.pallas_call(
        kernel,
        out_shape=out,
        in_specs=[smem] * len(scalars)
        + [far if n in hbm else vmem for n in range(len(operands))],
        out_specs=(vmem,) * len(out) if isinstance(out, tuple) else vmem,
        scratch_shapes=scratch,
        compiler_params=pltpu.CompilerParams(vmem_limit_bytes=limit),
        cost_estimate=pl.CostEstimate(flops=flops, bytes_accessed=moved, transcendentals=0),
    )(*(jnp.reshape(v, (1,)) for v in scalars), *operands)


def fetch(pairs, sems):
    copies = [pltpu.make_async_copy(a, b, sems.at[n]) for n, (a, b) in enumerate(pairs)]
    for copy in copies:
        copy.start()
    for copy in copies:
        copy.wait()


def pack_kernel(tokens_hbm, up_hbm, down_hbm, gain_hbm, out_ref, copies_ref, *scratch):
    tokens_ref, up_ref, down_ref, gain_ref, sems = scratch
    fetch(
        (
            (up_hbm, up_ref),
            (down_hbm, down_ref),
            (gain_hbm, gain_ref),
            (tokens_hbm, tokens_ref),
        ),
        sems,
    )
    cols = out_ref.shape[0]
    feats, width = up_ref.shape
    units = width // cols
    gain = gain_ref[...]
    first = gain.astype(bf16).astype(f32)
    second = (gain - first).astype(bf16).astype(f32)
    third = gain - first - second
    row = lax.broadcasted_iota(jnp.int32, (8, feats), 0)
    zero = jnp.zeros((8, feats), f32)
    rows = jnp.where(row == 0, first, jnp.where(row == 1, second, jnp.where(row == 2, third, zero)))
    rows = rows.astype(bf16)
    up = up_ref[...].astype(f32).T.astype(bf16)
    for j in range(cols):
        out_ref[j, :units] = up[j * units : (j + 1) * units]
        out_ref[j, units : 2 * units] = down_ref[j * units : (j + 1) * units]
        out_ref[j, 2 * units :] = rows
    tokens = tokens_ref[...]
    for k in range(copies_ref.shape[0]):
        copies_ref[k] = tokens


def unpack_kernel(arrived_ref, mine_ref):
    feats = arrived_ref.shape[2]
    both = mine_ref.shape[0]
    for j in range(arrived_ref.shape[0]):
        mine_ref[:, j * feats : (j + 1) * feats] = arrived_ref[j, :both]


def retention_kernel(decay_ref, *refs):
    sources, (shares_ref, keys_ref, values_ref) = refs[:11], refs[11:14]
    targets, (normed_ref, readout_ref, sems) = refs[14:25], refs[25:]
    copies = [
        pltpu.make_async_copy(a, b, sems.at[n]) for n, (a, b) in enumerate(zip(sources, targets))
    ]
    for copy in copies:
        copy.start()
    blocks_ref, mixer_ref, query_ref, key_ref, value_ref, gate_ref = targets[:6]
    cosine_ref, sine_ref, state_ref, output_ref, gain_ref = targets[6:]
    kv, served, feats = blocks_ref.shape
    for copy in copies[:2]:
        copy.wait()
    total = jnp.zeros((served, feats), f32)
    for k in range(kv):
        x = blocks_ref[k].astype(f32)
        total = total + x * x
    factor = lax.rsqrt(jnp.sum(total, axis=1, keepdims=True) / D + EPS)
    for k in range(kv):
        at = slice(k * feats, (k + 1) * feats)
        normed_ref[:, at] = (blocks_ref[k].astype(f32) * factor * mixer_ref[:, at]).astype(bf16)
    normed = normed_ref[...]
    middle = HEAD_DIM // 2

    def project(weight):
        return lax.dot_general(normed, weight, NT, preferred_element_type=f32)

    def rotated(ref):
        plain = project(ref[...])
        turned = project(jnp.concatenate([ref[middle:], ref[:middle]]))
        return plain * cosine_ref[...] + turned * sine_ref[...]

    for copy in copies[2:]:
        copy.wait()
    queries = rotated(query_ref)
    keys = rotated(key_ref) * HEAD_DIM ** (-0.5)
    values = project(value_ref[...])
    gating = project(gate_ref[...])
    keys_ref[...] = keys
    values_ref[...] = values
    columns = queries.T
    for b in range(state_ref.shape[0]):
        readout_ref[b : b + 1] = jnp.sum(state_ref[b] * columns[:, b : b + 1], axis=0, keepdims=True)
    matched = jnp.sum(keys * queries, axis=1, keepdims=True)
    readout = decay_ref[0] * readout_ref[...] + matched * values
    square = jnp.sum(readout * readout, axis=1, keepdims=True) / HEAD_DIM
    grouped = readout * lax.rsqrt(square + EPS) * gain_ref[...]
    merged = (grouped * (gating * jax.nn.sigmoid(gating))).astype(bf16)
    shares = jnp.dot(merged, output_ref[...], preferred_element_type=f32).astype(bf16)
    feats = shares_ref.shape[2]
    for k in range(shares_ref.shape[0]):
        shares_ref[k] = shares[:, k * feats : (k + 1) * feats]


def sum_of(parts_ref):
    total = parts_ref[0].astype(f32)
    for k in range(1, parts_ref.shape[0]):
        total = total + parts_ref[k].astype(f32)
    return total


def after_kernel(parts_ref, tokens_ref, out_ref):
    block = (tokens_ref[...].astype(f32) + sum_of(parts_ref)).astype(bf16)
    for p in range(out_ref.shape[0]):
        out_ref[p] = block


def up_kernel(rows_ref, arrived_ref, weights_ref, own_ref, sent_ref):
    cols, count, feats = rows_ref.shape
    lines = arrived_ref.shape[1]
    far, _, units, width = weights_ref.shape
    ones = jnp.ones((8, feats), bf16)
    total = jnp.zeros((8, count), f32)
    scaled = []
    for j in range(cols):
        x = rows_ref[j].astype(f32)
        pieces = arrived_ref[j, lines - 8 :].astype(f32)
        scaled.append((x * (pieces[0:1] + pieces[1:2] + pieces[2:3])).astype(bf16))
        square = x * x
        high = square.astype(bf16)
        low = (square - high.astype(f32)).astype(bf16)
        total = total + lax.dot_general(ones, high, NT, preferred_element_type=f32)
        total = total + lax.dot_general(ones, low, NT, preferred_element_type=f32)
    part = lax.dot_general(
        jnp.concatenate(scaled, axis=1),
        weights_ref[:, 0].reshape(far * units, width),
        NT,
        preferred_element_type=f32,
    )
    own_ref[:count] = part
    sent_ref[:count] = part.astype(bf16)
    high = total.astype(bf16).astype(f32)
    low = total - high
    row = lax.broadcasted_iota(jnp.int32, total.shape, 0)
    extra = jnp.where(row == 0, high, jnp.where(row == 1, low, jnp.zeros_like(total)))
    own_ref[count:] = extra
    sent_ref[count:] = extra.astype(bf16)


def down_kernel(own_ref, other_ref, weights_ref, out_ref):
    cols, count, feats = out_ref.shape
    total = own_ref[...] + other_ref[...].astype(f32)
    squares = total[count : count + 1] + total[count + 1 : count + 2]
    row = lax.broadcasted_iota(jnp.int32, (count, count), 0)
    lane = lax.broadcasted_iota(jnp.int32, (count, count), 1)
    mine = jnp.where(lane == row, squares, jnp.zeros((count, count), f32))
    factor = lax.rsqrt(jnp.sum(mine, axis=1, keepdims=True) / D + EPS)
    raised = jnp.maximum(total[:count] * factor, 0.0)
    hidden = (raised * raised).astype(bf16)
    weight = weights_ref[:, 1].reshape(-1, weights_ref.shape[3])
    part = jnp.dot(hidden, weight, preferred_element_type=f32).astype(bf16)
    for j in range(cols):
        out_ref[j] = part[:, j * feats : (j + 1) * feats]


def final_kernel(parts_ref, after_ref, out_ref):
    out_ref[...] = (after_ref[0].astype(f32) + sum_of(parts_ref)).astype(out_ref.dtype)


def layer(
    tokens,
    lengths,
    query_weight,
    key_weight,
    value_weight,
    gate_weight,
    output_weight,
    mixer_gain,
    group_gain,
    channel_gain,
    up_weight,
    down_weight,
    memory_state,
):
    like = jax.ShapeDtypeStruct
    served, feats = tokens.shape
    kv, cols, planes, far = size_of(KV), size_of(COLS), size_of(PLANES), size_of(FAR)
    units = up_weight.shape[1] // cols
    count = planes * served
    sent, copies = call(
        pack_kernel,
        (like((cols, 2 * units + 8, feats), bf16), like((kv, served, feats), bf16)),
        tokens,
        up_weight,
        down_weight,
        channel_gain.reshape(1, feats),
        hbm=(0, 1, 2, 3),
        limit=63 << 20,
        scratch=(
            pltpu.VMEM(tokens.shape, bf16),
            pltpu.VMEM(up_weight.shape, bf16),
            pltpu.VMEM(down_weight.shape, bf16),
            pltpu.VMEM((1, feats), f32),
            pltpu.SemaphoreType.DMA((4,)),
        ),
    )
    arrived = swap(sent, COLS)
    mine = call(unpack_kernel, like((2 * units, cols * feats), bf16), arrived)
    weights = lax.all_gather(mine, FAR, axis=0, tiled=True)

    blocks = swap(copies, KV)
    middle = HEAD_DIM // 2
    inverse = THETA ** (-jnp.arange(middle, dtype=f32) * 2.0 / HEAD_DIM)
    angles = lengths.astype(f32)[:, None] * inverse[None, :]
    cosine, sine = jnp.cos(angles), jnp.sin(angles)
    both_cosine = jnp.concatenate([cosine, cosine], axis=1)
    both_sine = jnp.concatenate([-sine, sine], axis=1)
    head = lax.axis_index(KV).astype(f32)
    decay = 1.0 - 2.0 ** (-5.0 - 5.0 * head / (HEADS - 1))
    state = memory_state[:, 0]
    operands = (
        blocks,
        mixer_gain.reshape(1, kv * feats),
        query_weight.T,
        key_weight.T,
        value_weight.T,
        gate_weight.T,
        both_cosine,
        both_sine,
        state,
        output_weight,
        group_gain.reshape(1, HEAD_DIM),
    )
    shares, keys_new, values_new = call(
        retention_kernel,
        (
            like((kv, served, feats), bf16),
            like((served, HEAD_DIM), f32),
            like((served, HEAD_DIM), f32),
        ),
        *operands,
        scalars=(decay,),
        hbm=tuple(range(len(operands))),
        scratch=(
            *(pltpu.VMEM(a.shape, a.dtype) for a in operands),
            pltpu.VMEM((served, kv * feats), bf16),
            pltpu.VMEM((served, HEAD_DIM), f32),
            pltpu.SemaphoreType.DMA((len(operands),)),
        ),
        limit=63 << 20,
        flops=2 * served * D * 6 * HEAD_DIM,
    )
    shares = swap(shares, KV)
    after = call(after_kernel, like((cols * planes, served, feats), bf16), shares, tokens)

    rows = swap(after, COLS + PLANES).reshape(cols, count, feats)
    weights = weights.reshape(far, 2, units, cols * feats)
    own, given = call(
        up_kernel,
        (
            like((count + 8, far * units), f32),
            like((count + 8, far * units), bf16),
        ),
        rows,
        arrived,
        weights,
        flops=2 * count * cols * feats * far * units,
    )
    other = lax.ppermute(given, HALF, [(0, 1), (1, 0)])
    lowered = call(
        down_kernel,
        like((cols, count, feats), bf16),
        own,
        other,
        weights,
        flops=2 * count * cols * feats * far * units,
    )

    lowered = swap(lowered.reshape(cols * planes, served, feats), COLS + PLANES)
    mixed = call(final_kernel, like((served, feats), bf16), lowered, after)
    new_state = decay * state + keys_new[:, :, None] * values_new[:, None, :]
    return (mixed, new_state[:, None])


def solution(mesh):
    fine = Mesh(mesh.devices.reshape(4, 2, 2, 2, 2, 2, 2, 2), KV + TP)
    return jax.shard_map(
        layer,
        mesh=fine,
        in_specs=(
            P(TP, KV),
            P(TP),
            P(None, KV),
            P(None, KV),
            P(None, KV),
            P(None, KV),
            P(KV, None),
            P(None),
            P(KV),
            P(KV),
            P(KV, TP),
            P(TP, KV),
            P(TP, KV, None, None),
        ),
        out_specs=(P(TP, KV), P(TP, KV, None, None)),
        check_vma=False,
    )
```

```python
import jax
import jax.numpy as jnp
import numpy as np
from jax import lax
from jax.experimental import pallas as pl
from jax.experimental.pallas import tpu as pltpu
from jax.sharding import Mesh
from jax.sharding import PartitionSpec as P

D = 2048
HEADS = 16
HEAD_DIM = 64
EPS = 1e-06
THETA = 10000.0

KV = ("y", "xh", "xl")
TP = ("b3", "b2", "b1", "b0", "c")
HALF = "xl"
COLS = ("y", "xh")
NEAR = "b0"
CORE = "c"
FAR = ("b3", "b2", "b1")

bf16, f32 = jnp.bfloat16, jnp.float32
NT = (((1,), (1,)), ((), ()))


def size_of(axes):
    return int(np.prod([lax.axis_size(a) for a in axes]))


def swap(blocks, axes):
    return lax.all_to_all(blocks, axes, split_axis=0, concat_axis=0, tiled=True)


def call(kernel, out, *operands, scalars=(), hbm=(), scratch=(), limit=16 << 20, flops=1 << 20):
    outs = out if isinstance(out, tuple) else (out,)
    moved = sum(o.size * o.dtype.itemsize for o in operands)
    moved += sum(int(np.prod(o.shape)) * o.dtype.itemsize for o in outs)
    smem = pl.BlockSpec(memory_space=pltpu.SMEM)
    vmem = pl.BlockSpec(memory_space=pltpu.VMEM)
    far = pl.BlockSpec(memory_space=pltpu.HBM)
    return pl.pallas_call(
        kernel,
        out_shape=out,
        in_specs=[smem] * len(scalars)
        + [far if n in hbm else vmem for n in range(len(operands))],
        out_specs=(vmem,) * len(out) if isinstance(out, tuple) else vmem,
        scratch_shapes=scratch,
        compiler_params=pltpu.CompilerParams(vmem_limit_bytes=limit),
        cost_estimate=pl.CostEstimate(flops=flops, bytes_accessed=moved, transcendentals=0),
    )(*(jnp.reshape(v, (1,)) for v in scalars), *operands)


def fetch(pairs, sems):
    copies = [pltpu.make_async_copy(a, b, sems.at[n]) for n, (a, b) in enumerate(pairs)]
    for copy in copies:
        copy.start()
    for copy in copies:
        copy.wait()


def pack_kernel(decay_ref, up_hbm, down_hbm, gain_hbm, out_ref, *scratch):
    up_ref, down_ref, gain_ref, sems = scratch
    fetch(
        (
            (up_hbm, up_ref),
            (down_hbm, down_ref),
            (gain_hbm, gain_ref),
        ),
        sems,
    )
    cols = out_ref.shape[0]
    feats, width = up_ref.shape
    units = width // cols
    gain = gain_ref[...]
    first = gain.astype(bf16).astype(f32)
    second = (gain - first).astype(bf16).astype(f32)
    third = gain - first - second
    row = lax.broadcasted_iota(jnp.int32, (8, feats), 0)
    zero = jnp.zeros((8, feats), f32)
    rows = jnp.where(row == 0, first, jnp.where(row == 1, second, jnp.where(row == 2, third, zero)))
    rows = rows.astype(bf16)
    up = up_ref[...].astype(f32).T.astype(bf16)
    for j in range(cols):
        out_ref[j, :units] = up[j * units : (j + 1) * units]
        out_ref[j, units : 2 * units] = down_ref[j * units : (j + 1) * units]
        out_ref[j, 2 * units :] = rows


def copies_kernel(tokens_ref, copies_ref):
    tokens = tokens_ref[...]
    for k in range(copies_ref.shape[0]):
        copies_ref[k] = tokens


def unpack_kernel(arrived_ref, mine_ref):
    feats = arrived_ref.shape[2]
    both = mine_ref.shape[0]
    for j in range(arrived_ref.shape[0]):
        mine_ref[:, j * feats : (j + 1) * feats] = arrived_ref[j, :both]


def retention_kernel(decay_ref, *refs):
    sources, (shares_ref, keys_ref, values_ref) = refs[:11], refs[11:14]
    targets, (normed_ref, readout_ref, sems) = refs[14:25], refs[25:]
    copies = [
        pltpu.make_async_copy(a, b, sems.at[n]) for n, (a, b) in enumerate(zip(sources, targets))
    ]
    for copy in copies:
        copy.start()
    blocks_ref, mixer_ref, query_ref, key_ref, value_ref, gate_ref = targets[:6]
    cosine_ref, sine_ref, state_ref, output_ref, gain_ref = targets[6:]
    kv, served, feats = blocks_ref.shape
    for copy in copies[:2]:
        copy.wait()
    total = jnp.zeros((served, feats), f32)
    for k in range(kv):
        x = blocks_ref[k].astype(f32)
        total = total + x * x
    factor = lax.rsqrt(jnp.sum(total, axis=1, keepdims=True) / D + EPS)
    for k in range(kv):
        at = slice(k * feats, (k + 1) * feats)
        normed_ref[:, at] = (blocks_ref[k].astype(f32) * factor * mixer_ref[:, at]).astype(bf16)
    normed = normed_ref[...]
    middle = HEAD_DIM // 2

    def project(weight):
        return lax.dot_general(normed, weight, NT, preferred_element_type=f32)

    def rotated(ref):
        plain = project(ref[...])
        turned = project(jnp.concatenate([ref[middle:], ref[:middle]]))
        return plain * cosine_ref[...] + turned * sine_ref[...]

    for copy in copies[2:8]:
        copy.wait()
    queries = rotated(query_ref)
    keys = rotated(key_ref) * HEAD_DIM ** (-0.5)
    values = project(value_ref[...])
    gating = project(gate_ref[...])
    keys_ref[...] = keys
    values_ref[...] = values
    columns = queries.T
    for copy in copies[8:]:
        copy.wait()
    for b in range(state_ref.shape[0]):
        readout_ref[b : b + 1] = jnp.sum(state_ref[b] * columns[:, b : b + 1], axis=0, keepdims=True)
    matched = jnp.sum(keys * queries, axis=1, keepdims=True)
    readout = decay_ref[0] * readout_ref[...] + matched * values
    square = jnp.sum(readout * readout, axis=1, keepdims=True) / HEAD_DIM
    grouped = readout * lax.rsqrt(square + EPS) * gain_ref[...]
    merged = (grouped * (gating * jax.nn.sigmoid(gating))).astype(bf16)
    shares = jnp.dot(merged, output_ref[...], preferred_element_type=f32).astype(bf16)
    feats = shares_ref.shape[2]
    for k in range(shares_ref.shape[0]):
        shares_ref[k] = shares[:, k * feats : (k + 1) * feats]


def sum_of(parts_ref):
    total = parts_ref[0].astype(f32)
    for k in range(1, parts_ref.shape[0]):
        total = total + parts_ref[k].astype(f32)
    return total


def after_kernel(parts_ref, tokens_ref, out_ref):
    out_ref[...] = (tokens_ref[...].astype(f32) + sum_of(parts_ref)).astype(bf16)


def rows_kernel(near_ref, own_ref, other_ref, out_ref):
    served = own_ref.shape[0]
    for n in range(2):
        block = jnp.where(near_ref[0] == n, own_ref[...], other_ref[...])
        for p in range(out_ref.shape[0]):
            out_ref[p, n * served : (n + 1) * served] = block


def up_kernel(rows_ref, arrived_ref, weights_ref, own_ref, sent_ref):
    cols, count, feats = rows_ref.shape
    lines = arrived_ref.shape[1]
    far, _, units, width = weights_ref.shape
    ones = jnp.ones((8, feats), bf16)
    total = jnp.zeros((8, count), f32)
    scaled = []
    for j in range(cols):
        x = rows_ref[j].astype(f32)
        pieces = arrived_ref[j, lines - 8 :].astype(f32)
        scaled.append((x * (pieces[0:1] + pieces[1:2] + pieces[2:3])).astype(bf16))
        square = x * x
        high = square.astype(bf16)
        low = (square - high.astype(f32)).astype(bf16)
        total = total + lax.dot_general(ones, high, NT, preferred_element_type=f32)
        total = total + lax.dot_general(ones, low, NT, preferred_element_type=f32)
    part = lax.dot_general(
        jnp.concatenate(scaled, axis=1),
        weights_ref[:, 0].reshape(far * units, width),
        NT,
        preferred_element_type=f32,
    )
    own_ref[:count] = part
    sent_ref[:count] = part.astype(bf16)
    high = total.astype(bf16).astype(f32)
    low = total - high
    row = lax.broadcasted_iota(jnp.int32, total.shape, 0)
    extra = jnp.where(row == 0, high, jnp.where(row == 1, low, jnp.zeros_like(total)))
    own_ref[count:] = extra
    sent_ref[count:] = extra.astype(bf16)


def down_kernel(own_ref, other_ref, weights_ref, out_ref):
    cols, count, feats = out_ref.shape
    total = own_ref[...] + other_ref[...].astype(f32)
    squares = total[count : count + 1] + total[count + 1 : count + 2]
    row = lax.broadcasted_iota(jnp.int32, (count, count), 0)
    lane = lax.broadcasted_iota(jnp.int32, (count, count), 1)
    mine = jnp.where(lane == row, squares, jnp.zeros((count, count), f32))
    factor = lax.rsqrt(jnp.sum(mine, axis=1, keepdims=True) / D + EPS)
    raised = jnp.maximum(total[:count] * factor, 0.0)
    hidden = (raised * raised).astype(bf16)
    weight = weights_ref[:, 1].reshape(-1, weights_ref.shape[3])
    part = jnp.dot(hidden, weight, preferred_element_type=f32).astype(bf16)
    for j in range(cols):
        out_ref[j] = part[:, j * feats : (j + 1) * feats]


def halves_kernel(near_ref, parts_ref, own_ref, sent_ref):
    served = own_ref.shape[0]
    total = sum_of(parts_ref)
    first, second = total[:served], total[served:]
    own_ref[...] = jnp.where(near_ref[0] == 0, first, second)
    sent_ref[...] = jnp.where(near_ref[0] == 0, second, first).astype(bf16)


def final_kernel(own_ref, other_ref, after_ref, out_ref):
    total = own_ref[...] + other_ref[...].astype(f32)
    out_ref[...] = (after_ref[...].astype(f32) + total).astype(out_ref.dtype)


def layer(
    tokens,
    lengths,
    query_weight,
    key_weight,
    value_weight,
    gate_weight,
    output_weight,
    mixer_gain,
    group_gain,
    channel_gain,
    up_weight,
    down_weight,
    memory_state,
):
    like = jax.ShapeDtypeStruct
    served, feats = tokens.shape
    kv, cols, far = size_of(KV), size_of(COLS), size_of(FAR)
    cores = lax.axis_size(CORE)
    units = up_weight.shape[1] // cols
    count = 2 * cores * served
    near = lax.axis_index(NEAR)
    turn = [(0, 1), (1, 0)]
    head = lax.axis_index(KV).astype(f32)
    decay = 1.0 - 2.0 ** (-5.0 - 5.0 * head / (HEADS - 1))
    sent = call(
        pack_kernel,
        like((cols, 2 * units + 8, feats), bf16),
        up_weight,
        down_weight,
        channel_gain.reshape(1, feats),
        scalars=(decay,),
        hbm=(0, 1, 2),
        limit=63 << 20,
        scratch=(
            pltpu.VMEM(up_weight.shape, bf16),
            pltpu.VMEM(down_weight.shape, bf16),
            pltpu.VMEM((1, feats), f32),
            pltpu.SemaphoreType.DMA((3,)),
        ),
    )
    arrived = swap(sent, COLS)
    mine = call(unpack_kernel, like((2 * units, cols * feats), bf16), arrived)
    weights = lax.all_gather(mine, FAR, axis=0, tiled=True)

    copies = call(copies_kernel, like((kv, served, feats), bf16), tokens)
    blocks = swap(copies, KV)
    middle = HEAD_DIM // 2
    inverse = THETA ** (-jnp.arange(middle, dtype=f32) * 2.0 / HEAD_DIM)
    angles = lengths.astype(f32)[:, None] * inverse[None, :]
    cosine, sine = jnp.cos(angles), jnp.sin(angles)
    both_cosine = jnp.concatenate([cosine, cosine], axis=1)
    both_sine = jnp.concatenate([-sine, sine], axis=1)
    state = memory_state[:, 0]
    operands = (
        blocks,
        mixer_gain.reshape(1, kv * feats),
        query_weight.T,
        key_weight.T,
        value_weight.T,
        gate_weight.T,
        both_cosine,
        both_sine,
        state,
        output_weight,
        group_gain.reshape(1, HEAD_DIM),
    )
    shares, keys_new, values_new = call(
        retention_kernel,
        (
            like((kv, served, feats), bf16),
            like((served, HEAD_DIM), f32),
            like((served, HEAD_DIM), f32),
        ),
        *operands,
        scalars=(decay,),
        hbm=tuple(range(len(operands))),
        scratch=(
            *(pltpu.VMEM(a.shape, a.dtype) for a in operands),
            pltpu.VMEM((served, kv * feats), bf16),
            pltpu.VMEM((served, HEAD_DIM), f32),
            pltpu.SemaphoreType.DMA((len(operands),)),
        ),
        limit=63 << 20,
        flops=2 * served * D * 6 * HEAD_DIM,
    )
    shares = swap(shares, KV)
    after = call(after_kernel, like((served, feats), bf16), shares, tokens)

    passed = lax.ppermute(after, NEAR, turn)
    copies = call(
        rows_kernel,
        like((cols * cores, 2 * served, feats), bf16),
        after,
        passed,
        scalars=(near,),
    )
    rows = swap(copies, COLS + (CORE,)).reshape(cols, count, feats)
    weights = weights.reshape(far, 2, units, cols * feats)
    own, given = call(
        up_kernel,
        (
            like((count + 8, far * units), f32),
            like((count + 8, far * units), bf16),
        ),
        rows,
        arrived,
        weights,
        flops=2 * count * cols * feats * far * units,
    )
    other = lax.ppermute(given, HALF, turn)
    lowered = call(
        down_kernel,
        like((cols, count, feats), bf16),
        own,
        other,
        weights,
        flops=2 * count * cols * feats * far * units,
    )

    lowered = swap(lowered.reshape(cols * cores, 2 * served, feats), COLS + (CORE,))
    kept, back = call(
        halves_kernel,
        (like((served, feats), f32), like((served, feats), bf16)),
        lowered,
        scalars=(near,),
    )
    returned = lax.ppermute(back, NEAR, turn)
    mixed = call(final_kernel, like((served, feats), bf16), kept, returned, after)
    new_state = decay * state + keys_new[:, :, None] * values_new[:, None, :]
    return (mixed, new_state[:, None])


def solution(mesh):
    fine = Mesh(mesh.devices.reshape(4, 2, 2, 2, 2, 2, 2, 2), KV + TP)
    return jax.shard_map(
        layer,
        mesh=fine,
        in_specs=(
            P(TP, KV),
            P(TP),
            P(None, KV),
            P(None, KV),
            P(None, KV),
            P(None, KV),
            P(KV, None),
            P(None),
            P(KV),
            P(KV),
            P(KV, TP),
            P(TP, KV),
            P(TP, KV, None, None),
        ),
        out_specs=(P(TP, KV), P(TP, KV, None, None)),
        check_vma=False,
    )
```

```python
import jax
import jax.numpy as jnp
import numpy as np
from jax import lax
from jax.experimental import pallas as pl
from jax.experimental.pallas import tpu as pltpu
from jax.sharding import Mesh
from jax.sharding import PartitionSpec as P

D = 2048
HEADS = 16
HEAD_DIM = 64
EPS = 1e-06
THETA = 10000.0

KV = ("y", "xh", "xl")
TP = ("b3", "b2", "b1", "b0", "c")
HALF = "xh"
COLS = ("y", "xl")
PLANES = ("b0", "c")
FAR = ("b3", "b2", "b1")

bf16, f32 = jnp.bfloat16, jnp.float32
NT = (((1,), (1,)), ((), ()))


def size_of(axes):
    return int(np.prod([lax.axis_size(a) for a in axes]))


def swap(blocks, axes):
    return lax.all_to_all(blocks, axes, split_axis=0, concat_axis=0, tiled=True)


def call(kernel, out, *operands, scalars=(), hbm=(), scratch=(), limit=16 << 20, flops=1 << 20):
    outs = out if isinstance(out, tuple) else (out,)
    moved = sum(o.size * o.dtype.itemsize for o in operands)
    moved += sum(int(np.prod(o.shape)) * o.dtype.itemsize for o in outs)
    smem = pl.BlockSpec(memory_space=pltpu.SMEM)
    vmem = pl.BlockSpec(memory_space=pltpu.VMEM)
    far = pl.BlockSpec(memory_space=pltpu.HBM)
    return pl.pallas_call(
        kernel,
        out_shape=out,
        in_specs=[smem] * len(scalars)
        + [far if n in hbm else vmem for n in range(len(operands))],
        out_specs=(vmem,) * len(out) if isinstance(out, tuple) else vmem,
        scratch_shapes=scratch,
        compiler_params=pltpu.CompilerParams(vmem_limit_bytes=limit),
        cost_estimate=pl.CostEstimate(flops=flops, bytes_accessed=moved, transcendentals=0),
    )(*(jnp.reshape(v, (1,)) for v in scalars), *operands)


def fetch(pairs, sems):
    copies = [pltpu.make_async_copy(a, b, sems.at[n]) for n, (a, b) in enumerate(pairs)]
    for copy in copies:
        copy.start()
    for copy in copies:
        copy.wait()


def pack_kernel(decay_ref, up_hbm, down_hbm, gain_hbm, out_ref, *scratch):
    up_ref, down_ref, gain_ref, sems = scratch
    fetch(
        (
            (up_hbm, up_ref),
            (down_hbm, down_ref),
            (gain_hbm, gain_ref),
        ),
        sems,
    )
    cols = out_ref.shape[0]
    feats, width = up_ref.shape
    units = width // cols
    gain = gain_ref[...]
    first = gain.astype(bf16).astype(f32)
    second = (gain - first).astype(bf16).astype(f32)
    third = gain - first - second
    row = lax.broadcasted_iota(jnp.int32, (8, feats), 0)
    zero = jnp.zeros((8, feats), f32)
    rows = jnp.where(row == 0, first, jnp.where(row == 1, second, jnp.where(row == 2, third, zero)))
    rows = rows.astype(bf16)
    up = up_ref[...].astype(f32).T.astype(bf16)
    for j in range(cols):
        out_ref[j, :units] = up[j * units : (j + 1) * units]
        out_ref[j, units : 2 * units] = down_ref[j * units : (j + 1) * units]
        out_ref[j, 2 * units :] = rows


def copies_kernel(tokens_ref, copies_ref):
    tokens = tokens_ref[...]
    for k in range(copies_ref.shape[0]):
        copies_ref[k] = tokens


def unpack_kernel(arrived_ref, mine_ref):
    feats = arrived_ref.shape[2]
    both = mine_ref.shape[0]
    for j in range(arrived_ref.shape[0]):
        mine_ref[:, j * feats : (j + 1) * feats] = arrived_ref[j, :both]


def retention_kernel(decay_ref, *refs):
    sources, (shares_ref, keys_ref, values_ref) = refs[:11], refs[11:14]
    targets, (normed_ref, readout_ref, sems) = refs[14:25], refs[25:]
    copies = [
        pltpu.make_async_copy(a, b, sems.at[n]) for n, (a, b) in enumerate(zip(sources, targets))
    ]
    for copy in copies:
        copy.start()
    blocks_ref, mixer_ref, query_ref, key_ref, value_ref, gate_ref = targets[:6]
    cosine_ref, sine_ref, state_ref, output_ref, gain_ref = targets[6:]
    kv, served, feats = blocks_ref.shape
    for copy in copies[:2]:
        copy.wait()
    total = jnp.zeros((served, feats), f32)
    for k in range(kv):
        x = blocks_ref[k].astype(f32)
        total = total + x * x
    factor = lax.rsqrt(jnp.sum(total, axis=1, keepdims=True) / D + EPS)
    for k in range(kv):
        at = slice(k * feats, (k + 1) * feats)
        normed_ref[:, at] = (blocks_ref[k].astype(f32) * factor * mixer_ref[:, at]).astype(bf16)
    normed = normed_ref[...]
    middle = HEAD_DIM // 2

    def project(weight):
        return lax.dot_general(normed, weight, NT, preferred_element_type=f32)

    def rotated(ref):
        plain = project(ref[...])
        turned = project(jnp.concatenate([ref[middle:], ref[:middle]]))
        return plain * cosine_ref[...] + turned * sine_ref[...]

    for copy in copies[2:8]:
        copy.wait()
    queries = rotated(query_ref)
    keys = rotated(key_ref) * HEAD_DIM ** (-0.5)
    values = project(value_ref[...])
    gating = project(gate_ref[...])
    keys_ref[...] = keys
    values_ref[...] = values
    columns = queries.T
    for copy in copies[8:]:
        copy.wait()
    for b in range(state_ref.shape[0]):
        readout_ref[b : b + 1] = jnp.sum(state_ref[b] * columns[:, b : b + 1], axis=0, keepdims=True)
    matched = jnp.sum(keys * queries, axis=1, keepdims=True)
    readout = decay_ref[0] * readout_ref[...] + matched * values
    square = jnp.sum(readout * readout, axis=1, keepdims=True) / HEAD_DIM
    grouped = readout * lax.rsqrt(square + EPS) * gain_ref[...]
    merged = (grouped * (gating * jax.nn.sigmoid(gating))).astype(bf16)
    shares = jnp.dot(merged, output_ref[...], preferred_element_type=f32).astype(bf16)
    feats = shares_ref.shape[2]
    for k in range(shares_ref.shape[0]):
        shares_ref[k] = shares[:, k * feats : (k + 1) * feats]


def sum_of(parts_ref):
    total = parts_ref[0].astype(f32)
    for k in range(1, parts_ref.shape[0]):
        total = total + parts_ref[k].astype(f32)
    return total


def after_kernel(parts_ref, tokens_ref, out_ref, one_ref):
    block = (tokens_ref[...].astype(f32) + sum_of(parts_ref)).astype(bf16)
    one_ref[...] = block
    for p in range(out_ref.shape[0]):
        out_ref[p] = block


def up_kernel(rows_ref, arrived_ref, weights_ref, own_ref, sent_ref):
    cols, count, feats = rows_ref.shape
    lines = arrived_ref.shape[1]
    far, _, units, width = weights_ref.shape
    ones = jnp.ones((8, feats), bf16)
    total = jnp.zeros((8, count), f32)
    scaled = []
    for j in range(cols):
        x = rows_ref[j].astype(f32)
        pieces = arrived_ref[j, lines - 8 :].astype(f32)
        scaled.append((x * (pieces[0:1] + pieces[1:2] + pieces[2:3])).astype(bf16))
        square = x * x
        high = square.astype(bf16)
        low = (square - high.astype(f32)).astype(bf16)
        total = total + lax.dot_general(ones, high, NT, preferred_element_type=f32)
        total = total + lax.dot_general(ones, low, NT, preferred_element_type=f32)
    part = lax.dot_general(
        jnp.concatenate(scaled, axis=1),
        weights_ref[:, 0].reshape(far * units, width),
        NT,
        preferred_element_type=f32,
    )
    own_ref[:count] = part
    sent_ref[:count] = part.astype(bf16)
    high = total.astype(bf16).astype(f32)
    low = total - high
    row = lax.broadcasted_iota(jnp.int32, total.shape, 0)
    extra = jnp.where(row == 0, high, jnp.where(row == 1, low, jnp.zeros_like(total)))
    own_ref[count:] = extra
    sent_ref[count:] = extra.astype(bf16)


def down_kernel(own_ref, other_ref, weights_ref, out_ref):
    cols, count, feats = out_ref.shape
    total = own_ref[...] + other_ref[...].astype(f32)
    squares = total[count : count + 1] + total[count + 1 : count + 2]
    row = lax.broadcasted_iota(jnp.int32, (count, count), 0)
    lane = lax.broadcasted_iota(jnp.int32, (count, count), 1)
    mine = jnp.where(lane == row, squares, jnp.zeros((count, count), f32))
    factor = lax.rsqrt(jnp.sum(mine, axis=1, keepdims=True) / D + EPS)
    raised = jnp.maximum(total[:count] * factor, 0.0)
    hidden = (raised * raised).astype(bf16)
    weight = weights_ref[:, 1].reshape(-1, weights_ref.shape[3])
    part = jnp.dot(hidden, weight, preferred_element_type=f32).astype(bf16)
    for j in range(cols):
        out_ref[j] = part[:, j * feats : (j + 1) * feats]


def final_kernel(parts_ref, after_ref, out_ref):
    out_ref[...] = (after_ref[...].astype(f32) + sum_of(parts_ref)).astype(out_ref.dtype)


def layer(
    tokens,
    lengths,
    query_weight,
    key_weight,
    value_weight,
    gate_weight,
    output_weight,
    mixer_gain,
    group_gain,
    channel_gain,
    up_weight,
    down_weight,
    memory_state,
):
    like = jax.ShapeDtypeStruct
    served, feats = tokens.shape
    kv, cols, planes, far = size_of(KV), size_of(COLS), size_of(PLANES), size_of(FAR)
    units = up_weight.shape[1] // cols
    count = planes * served
    head = lax.axis_index(KV).astype(f32)
    decay = 1.0 - 2.0 ** (-5.0 - 5.0 * head / (HEADS - 1))
    sent = call(
        pack_kernel,
        like((cols, 2 * units + 8, feats), bf16),
        up_weight,
        down_weight,
        channel_gain.reshape(1, feats),
        scalars=(decay,),
        hbm=(0, 1, 2),
        limit=63 << 20,
        scratch=(
            pltpu.VMEM(up_weight.shape, bf16),
            pltpu.VMEM(down_weight.shape, bf16),
            pltpu.VMEM((1, feats), f32),
            pltpu.SemaphoreType.DMA((3,)),
        ),
    )
    arrived = swap(sent, COLS)
    mine = call(unpack_kernel, like((2 * units, cols * feats), bf16), arrived)
    weights = lax.all_gather(mine, FAR, axis=0, tiled=True)

    copies = call(copies_kernel, like((kv, served, feats), bf16), tokens)
    blocks = swap(copies, KV)
    middle = HEAD_DIM // 2
    inverse = THETA ** (-jnp.arange(middle, dtype=f32) * 2.0 / HEAD_DIM)
    angles = lengths.astype(f32)[:, None] * inverse[None, :]
    cosine, sine = jnp.cos(angles), jnp.sin(angles)
    both_cosine = jnp.concatenate([cosine, cosine], axis=1)
    both_sine = jnp.concatenate([-sine, sine], axis=1)
    state = memory_state[:, 0]
    operands = (
        blocks,
        mixer_gain.reshape(1, kv * feats),
        query_weight.T,
        key_weight.T,
        value_weight.T,
        gate_weight.T,
        both_cosine,
        both_sine,
        state,
        output_weight,
        group_gain.reshape(1, HEAD_DIM),
    )
    shares, keys_new, values_new = call(
        retention_kernel,
        (
            like((kv, served, feats), bf16),
            like((served, HEAD_DIM), f32),
            like((served, HEAD_DIM), f32),
        ),
        *operands,
        scalars=(decay,),
        hbm=tuple(range(len(operands))),
        scratch=(
            *(pltpu.VMEM(a.shape, a.dtype) for a in operands),
            pltpu.VMEM((served, kv * feats), bf16),
            pltpu.VMEM((served, HEAD_DIM), f32),
            pltpu.SemaphoreType.DMA((len(operands),)),
        ),
        limit=63 << 20,
        flops=2 * served * D * 6 * HEAD_DIM,
    )
    shares = swap(shares, KV)
    copies, after = call(
        after_kernel,
        (like((cols * planes, served, feats), bf16), like((served, feats), bf16)),
        shares,
        tokens,
    )

    rows = swap(copies, COLS + PLANES).reshape(cols, count, feats)
    weights = weights.reshape(far, 2, units, cols * feats)
    own, given = call(
        up_kernel,
        (
            like((count + 8, far * units), f32),
            like((count + 8, far * units), bf16),
        ),
        rows,
        arrived,
        weights,
        flops=2 * count * cols * feats * far * units,
    )
    other = lax.ppermute(given, HALF, [(0, 1), (1, 0)])
    lowered = call(
        down_kernel,
        like((cols, count, feats), bf16),
        own,
        other,
        weights,
        flops=2 * count * cols * feats * far * units,
    )

    lowered = swap(lowered.reshape(cols * planes, served, feats), COLS + PLANES)
    mixed = call(final_kernel, like((served, feats), bf16), lowered, after)
    new_state = decay * state + keys_new[:, :, None] * values_new[:, None, :]
    return (mixed, new_state[:, None])


def solution(mesh):
    fine = Mesh(mesh.devices.reshape(4, 2, 2, 2, 2, 2, 2, 2), KV + TP)
    return jax.shard_map(
        layer,
        mesh=fine,
        in_specs=(
            P(TP, KV),
            P(TP),
            P(None, KV),
            P(None, KV),
            P(None, KV),
            P(None, KV),
            P(KV, None),
            P(None),
            P(KV),
            P(KV),
            P(KV, TP),
            P(TP, KV),
            P(TP, KV, None, None),
        ),
        out_specs=(P(TP, KV), P(TP, KV, None, None)),
        check_vma=False,
    )
```

```python
import jax
import jax.numpy as jnp
import numpy as np
from jax import lax
from jax.experimental import pallas as pl
from jax.experimental.pallas import tpu as pltpu
from jax.sharding import Mesh
from jax.sharding import PartitionSpec as P

D = 2048
HEADS = 16
HEAD_DIM = 64
EPS = 1e-06
THETA = 10000.0

KV = ("y", "xh", "xl")
TP = ("b3", "b2", "b1", "b0", "c")
HALF = "xh"
COLS = ("y", "xl")
NEAR = "b0"
CORE = "c"
FAR = ("b3", "b2", "b1")

bf16, f32 = jnp.bfloat16, jnp.float32
NT = (((1,), (1,)), ((), ()))


def size_of(axes):
    return int(np.prod([lax.axis_size(a) for a in axes]))


def swap(blocks, axes):
    return lax.all_to_all(blocks, axes, split_axis=0, concat_axis=0, tiled=True)


def call(kernel, out, *operands, scalars=(), hbm=(), out_hbm=(), scratch=(), limit=16 << 20, flops=1 << 20):
    outs = out if isinstance(out, tuple) else (out,)
    moved = sum(o.size * o.dtype.itemsize for o in operands)
    moved += sum(int(np.prod(o.shape)) * o.dtype.itemsize for o in outs)
    smem = pl.BlockSpec(memory_space=pltpu.SMEM)
    vmem = pl.BlockSpec(memory_space=pltpu.VMEM)
    far = pl.BlockSpec(memory_space=pltpu.HBM)
    return pl.pallas_call(
        kernel,
        out_shape=out,
        in_specs=[smem] * len(scalars)
        + [far if n in hbm else vmem for n in range(len(operands))],
        out_specs=tuple(far if n in out_hbm else vmem for n in range(len(out)))
        if isinstance(out, tuple)
        else vmem,
        scratch_shapes=scratch,
        compiler_params=pltpu.CompilerParams(vmem_limit_bytes=limit),
        cost_estimate=pl.CostEstimate(flops=flops, bytes_accessed=moved, transcendentals=0),
    )(*(jnp.reshape(v, (1,)) for v in scalars), *operands)


def fetch(pairs, sems):
    copies = [pltpu.make_async_copy(a, b, sems.at[n]) for n, (a, b) in enumerate(pairs)]
    for copy in copies:
        copy.start()
    for copy in copies:
        copy.wait()


def pack_kernel(decay_ref, up_hbm, down_hbm, gain_hbm, out_ref, *scratch):
    up_ref, down_ref, gain_ref, sems = scratch
    fetch(
        (
            (up_hbm, up_ref),
            (down_hbm, down_ref),
            (gain_hbm, gain_ref),
        ),
        sems,
    )
    cols = out_ref.shape[0]
    feats, width = up_ref.shape
    units = width // cols
    gain = gain_ref[...]
    first = gain.astype(bf16).astype(f32)
    second = (gain - first).astype(bf16).astype(f32)
    third = gain - first - second
    row = lax.broadcasted_iota(jnp.int32, (8, feats), 0)
    zero = jnp.zeros((8, feats), f32)
    rows = jnp.where(row == 0, first, jnp.where(row == 1, second, jnp.where(row == 2, third, zero)))
    rows = rows.astype(bf16)
    up = up_ref[...].astype(f32).T.astype(bf16)
    for j in range(cols):
        out_ref[j, :units] = up[j * units : (j + 1) * units]
        out_ref[j, units : 2 * units] = down_ref[j * units : (j + 1) * units]
        out_ref[j, 2 * units :] = rows


def copies_kernel(tokens_ref, copies_ref):
    tokens = tokens_ref[...]
    for k in range(copies_ref.shape[0]):
        copies_ref[k] = tokens


def unpack_kernel(arrived_ref, mine_ref):
    feats = arrived_ref.shape[2]
    both = mine_ref.shape[0]
    for j in range(arrived_ref.shape[0]):
        mine_ref[:, j * feats : (j + 1) * feats] = arrived_ref[j, :both]


def retention_kernel(decay_ref, *refs):
    sources, (shares_ref, new_hbm) = refs[:11], refs[11:13]
    targets, (normed_ref, readout_ref, new_ref, sems, out_sems) = refs[13:24], refs[24:]
    copies = [
        pltpu.make_async_copy(a, b, sems.at[n]) for n, (a, b) in enumerate(zip(sources, targets))
    ]
    for copy in copies:
        copy.start()
    blocks_ref, mixer_ref, query_ref, key_ref, value_ref, gate_ref = targets[:6]
    cosine_ref, sine_ref, state_ref, output_ref, gain_ref = targets[6:]
    kv, served, feats = blocks_ref.shape
    for copy in copies[:2]:
        copy.wait()
    total = jnp.zeros((served, feats), f32)
    for k in range(kv):
        x = blocks_ref[k].astype(f32)
        total = total + x * x
    factor = lax.rsqrt(jnp.sum(total, axis=1, keepdims=True) / D + EPS)
    for k in range(kv):
        at = slice(k * feats, (k + 1) * feats)
        normed_ref[:, at] = (blocks_ref[k].astype(f32) * factor * mixer_ref[:, at]).astype(bf16)
    normed = normed_ref[...]
    middle = HEAD_DIM // 2

    def project(weight):
        return lax.dot_general(normed, weight, NT, preferred_element_type=f32)

    def rotated(ref):
        plain = project(ref[...])
        turned = project(jnp.concatenate([ref[middle:], ref[:middle]]))
        return plain * cosine_ref[...] + turned * sine_ref[...]

    for copy in copies[2:8]:
        copy.wait()
    queries = rotated(query_ref)
    keys = rotated(key_ref) * HEAD_DIM ** (-0.5)
    values = project(value_ref[...])
    gating = project(gate_ref[...])
    columns, key_columns = queries.T, keys.T
    for copy in copies[8:]:
        copy.wait()
    step = served // out_sems.shape[0]
    given = [
        pltpu.make_async_copy(
            new_ref.at[pl.ds(n * step, step)], new_hbm.at[pl.ds(n * step, step)], out_sems.at[n]
        )
        for n in range(out_sems.shape[0])
    ]
    for b in range(served):
        added = key_columns[:, b : b + 1] * values[b : b + 1]
        new_ref[b] = decay_ref[0] * state_ref[b] + added
        if b % step == step - 1 and b > step:
            given[b // step - 1].start()
    for b in range(state_ref.shape[0]):
        readout_ref[b : b + 1] = jnp.sum(state_ref[b] * columns[:, b : b + 1], axis=0, keepdims=True)
    matched = jnp.sum(keys * queries, axis=1, keepdims=True)
    readout = decay_ref[0] * readout_ref[...] + matched * values
    square = jnp.sum(readout * readout, axis=1, keepdims=True) / HEAD_DIM
    grouped = readout * lax.rsqrt(square + EPS) * gain_ref[...]
    merged = (grouped * (gating * jax.nn.sigmoid(gating))).astype(bf16)
    shares = jnp.dot(merged, output_ref[...], preferred_element_type=f32).astype(bf16)
    for k in range(shares_ref.shape[0]):
        shares_ref[k] = shares[:, k * feats : (k + 1) * feats]
    given[-1].start()
    for copy in given:
        copy.wait()


def sum_of(parts_ref):
    total = parts_ref[0].astype(f32)
    for k in range(1, parts_ref.shape[0]):
        total = total + parts_ref[k].astype(f32)
    return total


def after_kernel(parts_ref, tokens_ref, out_ref):
    out_ref[...] = (tokens_ref[...].astype(f32) + sum_of(parts_ref)).astype(bf16)


def rows_kernel(near_ref, own_ref, other_ref, out_ref):
    served = own_ref.shape[0]
    for n in range(2):
        block = jnp.where(near_ref[0] == n, own_ref[...], other_ref[...])
        for p in range(out_ref.shape[0]):
            out_ref[p, n * served : (n + 1) * served] = block


def up_kernel(rows_ref, arrived_ref, weights_ref, own_ref, sent_ref):
    cols, count, feats = rows_ref.shape
    lines = arrived_ref.shape[1]
    far, _, units, width = weights_ref.shape
    ones = jnp.ones((8, feats), bf16)
    total = jnp.zeros((8, count), f32)
    scaled = []
    for j in range(cols):
        x = rows_ref[j].astype(f32)
        pieces = arrived_ref[j, lines - 8 :].astype(f32)
        scaled.append((x * (pieces[0:1] + pieces[1:2] + pieces[2:3])).astype(bf16))
        square = x * x
        high = square.astype(bf16)
        low = (square - high.astype(f32)).astype(bf16)
        total = total + lax.dot_general(ones, high, NT, preferred_element_type=f32)
        total = total + lax.dot_general(ones, low, NT, preferred_element_type=f32)
    part = lax.dot_general(
        jnp.concatenate(scaled, axis=1),
        weights_ref[:, 0].reshape(far * units, width),
        NT,
        preferred_element_type=f32,
    )
    own_ref[:count] = part
    sent_ref[:count] = part.astype(bf16)
    high = total.astype(bf16).astype(f32)
    low = total - high
    row = lax.broadcasted_iota(jnp.int32, total.shape, 0)
    extra = jnp.where(row == 0, high, jnp.where(row == 1, low, jnp.zeros_like(total)))
    own_ref[count:] = extra
    sent_ref[count:] = extra.astype(bf16)


def down_kernel(own_ref, other_ref, weights_ref, out_ref):
    cols, count, feats = out_ref.shape
    total = own_ref[...] + other_ref[...].astype(f32)
    squares = total[count : count + 1] + total[count + 1 : count + 2]
    row = lax.broadcasted_iota(jnp.int32, (count, count), 0)
    lane = lax.broadcasted_iota(jnp.int32, (count, count), 1)
    mine = jnp.where(lane == row, squares, jnp.zeros((count, count), f32))
    factor = lax.rsqrt(jnp.sum(mine, axis=1, keepdims=True) / D + EPS)
    raised = jnp.maximum(total[:count] * factor, 0.0)
    hidden = (raised * raised).astype(bf16)
    weight = weights_ref[:, 1].reshape(-1, weights_ref.shape[3])
    part = jnp.dot(hidden, weight, preferred_element_type=f32).astype(bf16)
    for j in range(cols):
        out_ref[j] = part[:, j * feats : (j + 1) * feats]


def final_kernel(parts_ref, after_ref, out_ref):
    out_ref[...] = (after_ref[...].astype(f32) + sum_of(parts_ref)).astype(out_ref.dtype)


def layer(
    tokens,
    lengths,
    query_weight,
    key_weight,
    value_weight,
    gate_weight,
    output_weight,
    mixer_gain,
    group_gain,
    channel_gain,
    up_weight,
    down_weight,
    memory_state,
):
    like = jax.ShapeDtypeStruct
    served, feats = tokens.shape
    kv, cols, far = size_of(KV), size_of(COLS), size_of(FAR)
    cores = lax.axis_size(CORE)
    units = up_weight.shape[1] // cols
    count = 2 * cores * served
    near = lax.axis_index(NEAR)
    turn = [(0, 1), (1, 0)]
    head = lax.axis_index(KV).astype(f32)
    decay = 1.0 - 2.0 ** (-5.0 - 5.0 * head / (HEADS - 1))
    sent = call(
        pack_kernel,
        like((cols, 2 * units + 8, feats), bf16),
        up_weight,
        down_weight,
        channel_gain.reshape(1, feats),
        scalars=(decay,),
        hbm=(0, 1, 2),
        limit=63 << 20,
        scratch=(
            pltpu.VMEM(up_weight.shape, bf16),
            pltpu.VMEM(down_weight.shape, bf16),
            pltpu.VMEM((1, feats), f32),
            pltpu.SemaphoreType.DMA((3,)),
        ),
    )
    arrived = swap(sent, COLS)
    mine = call(unpack_kernel, like((2 * units, cols * feats), bf16), arrived)
    weights = lax.all_gather(mine, FAR, axis=0, tiled=True)

    copies = call(copies_kernel, like((kv, served, feats), bf16), tokens)
    blocks = swap(copies, KV)
    middle = HEAD_DIM // 2
    inverse = THETA ** (-jnp.arange(middle, dtype=f32) * 2.0 / HEAD_DIM)
    angles = lengths.astype(f32)[:, None] * inverse[None, :]
    cosine, sine = jnp.cos(angles), jnp.sin(angles)
    both_cosine = jnp.concatenate([cosine, cosine], axis=1)
    both_sine = jnp.concatenate([-sine, sine], axis=1)
    state = memory_state[:, 0]
    operands = (
        blocks,
        mixer_gain.reshape(1, kv * feats),
        query_weight.T,
        key_weight.T,
        value_weight.T,
        gate_weight.T,
        both_cosine,
        both_sine,
        state,
        output_weight,
        group_gain.reshape(1, HEAD_DIM),
    )
    shares, new_state = call(
        retention_kernel,
        (like((kv, served, feats), bf16), like(state.shape, f32)),
        *operands,
        scalars=(decay,),
        hbm=tuple(range(len(operands))),
        out_hbm=(1,),
        scratch=(
            *(pltpu.VMEM(a.shape, a.dtype) for a in operands),
            pltpu.VMEM((served, kv * feats), bf16),
            pltpu.VMEM((served, HEAD_DIM), f32),
            pltpu.VMEM(state.shape, f32),
            pltpu.SemaphoreType.DMA((len(operands),)),
            pltpu.SemaphoreType.DMA((4,)),
        ),
        limit=63 << 20,
        flops=2 * served * D * 6 * HEAD_DIM,
    )
    shares = swap(shares, KV)
    after = call(after_kernel, like((served, feats), bf16), shares, tokens)

    passed = lax.ppermute(after, NEAR, turn)
    copies = call(
        rows_kernel,
        like((cols * cores, 2 * served, feats), bf16),
        after,
        passed,
        scalars=(near,),
    )
    rows = swap(copies, COLS + (CORE,)).reshape(cols, count, feats)
    weights = weights.reshape(far, 2, units, cols * feats)
    own, given = call(
        up_kernel,
        (
            like((count + 8, far * units), f32),
            like((count + 8, far * units), bf16),
        ),
        rows,
        arrived,
        weights,
        flops=2 * count * cols * feats * far * units,
    )
    other = lax.ppermute(given, HALF, turn)
    lowered = call(
        down_kernel,
        like((cols, count, feats), bf16),
        own,
        other,
        weights,
        flops=2 * count * cols * feats * far * units,
    )

    lowered = lowered.reshape(cols * 2 * cores, served, feats)
    lowered = swap(lowered, COLS + (CORE, NEAR))
    mixed = call(final_kernel, like((served, feats), bf16), lowered, after)
    return (mixed, new_state[:, None])


def solution(mesh):
    fine = Mesh(mesh.devices.reshape(4, 2, 2, 2, 2, 2, 2, 2), KV + TP)
    return jax.shard_map(
        layer,
        mesh=fine,
        in_specs=(
            P(TP, KV),
            P(TP),
            P(None, KV),
            P(None, KV),
            P(None, KV),
            P(None, KV),
            P(KV, None),
            P(None),
            P(KV),
            P(KV),
            P(KV, TP),
            P(TP, KV),
            P(TP, KV, None, None),
        ),
        out_specs=(P(TP, KV), P(TP, KV, None, None)),
        check_vma=False,
    )
```

```python
import jax
import jax.numpy as jnp
import numpy as np
from jax import lax
from jax.experimental import pallas as pl
from jax.experimental.pallas import tpu as pltpu
from jax.sharding import Mesh
from jax.sharding import PartitionSpec as P

D = 2048
HEADS = 16
HEAD_DIM = 64
EPS = 1e-06
THETA = 10000.0

KV = ("y", "xh", "xl")
TP = ("b3", "b2", "b1", "b0", "c")
HALF = "xh"
COLS = ("y", "xl")
RING = ("xh", "xl")
NEAR = "b0"
CORE = "c"
FAR = ("b3", "b2", "b1")

bf16, f32 = jnp.bfloat16, jnp.float32
NT = (((1,), (1,)), ((), ()))


def size_of(axes):
    return int(np.prod([lax.axis_size(a) for a in axes]))


def swap(blocks, axes):
    return lax.all_to_all(blocks, axes, split_axis=0, concat_axis=0, tiled=True)


def call(kernel, out, *operands, scalars=(), hbm=(), out_hbm=(), scratch=(), limit=16 << 20, flops=1 << 20):
    outs = out if isinstance(out, tuple) else (out,)
    moved = sum(o.size * o.dtype.itemsize for o in operands)
    moved += sum(int(np.prod(o.shape)) * o.dtype.itemsize for o in outs)
    smem = pl.BlockSpec(memory_space=pltpu.SMEM)
    vmem = pl.BlockSpec(memory_space=pltpu.VMEM)
    far = pl.BlockSpec(memory_space=pltpu.HBM)
    return pl.pallas_call(
        kernel,
        out_shape=out,
        in_specs=[smem] * len(scalars)
        + [far if n in hbm else vmem for n in range(len(operands))],
        out_specs=tuple(far if n in out_hbm else vmem for n in range(len(out)))
        if isinstance(out, tuple)
        else vmem,
        scratch_shapes=scratch,
        compiler_params=pltpu.CompilerParams(vmem_limit_bytes=limit),
        cost_estimate=pl.CostEstimate(flops=flops, bytes_accessed=moved, transcendentals=0),
    )(*(jnp.reshape(v, (1,)) for v in scalars), *operands)


def fetch(pairs, sems):
    copies = [pltpu.make_async_copy(a, b, sems.at[n]) for n, (a, b) in enumerate(pairs)]
    for copy in copies:
        copy.start()
    for copy in copies:
        copy.wait()


def pack_kernel(decay_ref, half_ref, up_hbm, down_hbm, gain_hbm, out_ref, *scratch):
    up_ref, down_ref, gain_ref, sems = scratch
    fetch(
        (
            (up_hbm, up_ref),
            (down_hbm, down_ref),
            (gain_hbm, gain_ref),
        ),
        sems,
    )
    cols = out_ref.shape[0]
    feats, width = up_ref.shape
    units = width // cols
    gain = gain_ref[...]
    first = gain.astype(bf16).astype(f32)
    second = (gain - first).astype(bf16).astype(f32)
    third = gain - first - second
    row = lax.broadcasted_iota(jnp.int32, (8, feats), 0)
    zero = jnp.zeros((8, feats), f32)
    rows = jnp.where(row == 0, first, jnp.where(row == 1, second, jnp.where(row == 2, third, zero)))
    rows = rows.astype(bf16)
    up = up_ref[...].astype(f32).T.astype(bf16)
    down = down_ref[...]
    for j in range(cols):
        at, turned = slice(j * units, (j + 1) * units), slice((j ^ 1) * units, ((j ^ 1) + 1) * units)
        out_ref[j, :units] = jnp.where(half_ref[0] == 0, up[at], up[turned])
        out_ref[j, units : 2 * units] = jnp.where(half_ref[0] == 0, down[at], down[turned])
        out_ref[j, 2 * units :] = rows


def copies_kernel(tokens_ref, copies_ref):
    tokens = tokens_ref[...]
    for k in range(copies_ref.shape[0]):
        copies_ref[k] = tokens


def retention_kernel(decay_ref, *refs):
    sources, (shares_ref, new_hbm) = refs[:11], refs[11:13]
    targets, (normed_ref, readout_ref, new_ref, sems, out_sems) = refs[13:24], refs[24:]
    copies = [
        pltpu.make_async_copy(a, b, sems.at[n]) for n, (a, b) in enumerate(zip(sources, targets))
    ]
    for copy in copies:
        copy.start()
    blocks_ref, mixer_ref, query_ref, key_ref, value_ref, gate_ref = targets[:6]
    cosine_ref, sine_ref, state_ref, output_ref, gain_ref = targets[6:]
    kv, served, feats = blocks_ref.shape
    for copy in copies[:2]:
        copy.wait()
    total = jnp.zeros((served, feats), f32)
    for k in range(kv):
        x = blocks_ref[k].astype(f32)
        total = total + x * x
    factor = lax.rsqrt(jnp.sum(total, axis=1, keepdims=True) / D + EPS)
    for k in range(kv):
        at = slice(k * feats, (k + 1) * feats)
        normed_ref[:, at] = (blocks_ref[k].astype(f32) * factor * mixer_ref[:, at]).astype(bf16)
    normed = normed_ref[...]
    middle = HEAD_DIM // 2

    def project(weight):
        return lax.dot_general(normed, weight, NT, preferred_element_type=f32)

    def rotated(ref):
        plain = project(ref[...])
        turned = project(jnp.concatenate([ref[middle:], ref[:middle]]))
        return plain * cosine_ref[...] + turned * sine_ref[...]

    for copy in copies[2:8]:
        copy.wait()
    queries = rotated(query_ref)
    keys = rotated(key_ref) * HEAD_DIM ** (-0.5)
    values = project(value_ref[...])
    gating = project(gate_ref[...])
    columns, key_columns = queries.T, keys.T
    for copy in copies[8:]:
        copy.wait()
    step = served // out_sems.shape[0]
    given = [
        pltpu.make_async_copy(
            new_ref.at[pl.ds(n * step, step)], new_hbm.at[pl.ds(n * step, step)], out_sems.at[n]
        )
        for n in range(out_sems.shape[0])
    ]
    for b in range(served):
        added = key_columns[:, b : b + 1] * values[b : b + 1]
        new_ref[b] = decay_ref[0] * state_ref[b] + added
        if b % step == step - 1 and b > step:
            given[b // step - 1].start()
    for b in range(state_ref.shape[0]):
        readout_ref[b : b + 1] = jnp.sum(state_ref[b] * columns[:, b : b + 1], axis=0, keepdims=True)
    matched = jnp.sum(keys * queries, axis=1, keepdims=True)
    readout = decay_ref[0] * readout_ref[...] + matched * values
    square = jnp.sum(readout * readout, axis=1, keepdims=True) / HEAD_DIM
    grouped = readout * lax.rsqrt(square + EPS) * gain_ref[...]
    merged = (grouped * (gating * jax.nn.sigmoid(gating))).astype(bf16)
    shares = jnp.dot(merged, output_ref[...], preferred_element_type=f32).astype(bf16)
    for k in range(shares_ref.shape[0]):
        shares_ref[k] = shares[:, k * feats : (k + 1) * feats]
    given[-1].start()
    for copy in given:
        copy.wait()


def sum_of(parts_ref):
    total = parts_ref[0].astype(f32)
    for k in range(1, parts_ref.shape[0]):
        total = total + parts_ref[k].astype(f32)
    return total


def after_kernel(parts_ref, tokens_ref, out_ref):
    out_ref[...] = (tokens_ref[...].astype(f32) + sum_of(parts_ref)).astype(bf16)


def rows_kernel(near_ref, own_ref, other_ref, out_ref):
    served = own_ref.shape[0]
    for n in range(2):
        block = jnp.where(near_ref[0] == n, own_ref[...], other_ref[...])
        for p in range(out_ref.shape[0]):
            out_ref[p, n * served : (n + 1) * served] = block


def up_kernel(rows_ref, arrived_ref, weights_ref, own_ref, sent_ref):
    cols, count, feats = rows_ref.shape
    lines = arrived_ref.shape[1]
    far = weights_ref.shape[0] // cols
    part = jnp.zeros((count, sent_ref.shape[1]), f32)
    ones = jnp.ones((8, feats), bf16)
    total = jnp.zeros((8, count), f32)
    for j in range(cols):
        x = rows_ref[j].astype(f32)
        pieces = arrived_ref[j, lines - 8 :].astype(f32)
        scaled = (x * (pieces[0:1] + pieces[1:2] + pieces[2:3])).astype(bf16)
        weight = jnp.concatenate([weights_ref[f * cols + j] for f in range(far)])
        part = part + lax.dot_general(scaled, weight, NT, preferred_element_type=f32)
        square = x * x
        high = square.astype(bf16)
        low = (square - high.astype(f32)).astype(bf16)
        total = total + lax.dot_general(ones, high, NT, preferred_element_type=f32)
        total = total + lax.dot_general(ones, low, NT, preferred_element_type=f32)
    own_ref[:count] = part
    sent_ref[:count] = part.astype(bf16)
    high = total.astype(bf16).astype(f32)
    low = total - high
    row = lax.broadcasted_iota(jnp.int32, total.shape, 0)
    extra = jnp.where(row == 0, high, jnp.where(row == 1, low, jnp.zeros_like(total)))
    own_ref[count:] = extra
    sent_ref[count:] = extra.astype(bf16)


def down_kernel(own_ref, other_ref, weights_ref, out_ref):
    cols, count, _ = out_ref.shape
    total = own_ref[...] + other_ref[...].astype(f32)
    squares = total[count : count + 1] + total[count + 1 : count + 2]
    row = lax.broadcasted_iota(jnp.int32, (count, count), 0)
    lane = lax.broadcasted_iota(jnp.int32, (count, count), 1)
    mine = jnp.where(lane == row, squares, jnp.zeros((count, count), f32))
    factor = lax.rsqrt(jnp.sum(mine, axis=1, keepdims=True) / D + EPS)
    raised = jnp.maximum(total[:count] * factor, 0.0)
    hidden = (raised * raised).astype(bf16)
    far = weights_ref.shape[0] // cols
    for j in range(cols):
        weight = jnp.concatenate([weights_ref[f * cols + j] for f in range(far)])
        out_ref[j] = jnp.dot(hidden, weight, preferred_element_type=f32).astype(bf16)


def final_kernel(parts_ref, after_ref, out_ref):
    out_ref[...] = (after_ref[...].astype(f32) + sum_of(parts_ref)).astype(out_ref.dtype)


def layer(
    tokens,
    lengths,
    query_weight,
    key_weight,
    value_weight,
    gate_weight,
    output_weight,
    mixer_gain,
    group_gain,
    channel_gain,
    up_weight,
    down_weight,
    memory_state,
):
    like = jax.ShapeDtypeStruct
    served, feats = tokens.shape
    kv, cols, far = size_of(KV), size_of(COLS), size_of(FAR)
    cores = lax.axis_size(CORE)
    units = up_weight.shape[1] // cols
    count = 2 * cores * served
    near = lax.axis_index(NEAR)
    turn = [(0, 1), (1, 0)]
    head = lax.axis_index(KV).astype(f32)
    decay = 1.0 - 2.0 ** (-5.0 - 5.0 * head / (HEADS - 1))
    sent = call(
        pack_kernel,
        like((cols, 2 * units + 8, feats), bf16),
        up_weight,
        down_weight,
        channel_gain.reshape(1, feats),
        scalars=(decay, lax.axis_index(HALF)),
        hbm=(0, 1, 2),
        limit=63 << 20,
        scratch=(
            pltpu.VMEM(up_weight.shape, bf16),
            pltpu.VMEM(down_weight.shape, bf16),
            pltpu.VMEM((1, feats), f32),
            pltpu.SemaphoreType.DMA((3,)),
        ),
    )
    arrived = swap(sent, COLS)
    weights = lax.all_gather(arrived, FAR, axis=0, tiled=True)

    copies = call(copies_kernel, like((kv, served, feats), bf16), tokens)
    blocks = swap(copies, KV)
    middle = HEAD_DIM // 2
    inverse = THETA ** (-jnp.arange(middle, dtype=f32) * 2.0 / HEAD_DIM)
    angles = lengths.astype(f32)[:, None] * inverse[None, :]
    cosine, sine = jnp.cos(angles), jnp.sin(angles)
    both_cosine = jnp.concatenate([cosine, cosine], axis=1)
    both_sine = jnp.concatenate([-sine, sine], axis=1)
    state = memory_state[:, 0]
    operands = (
        blocks,
        mixer_gain.reshape(1, kv * feats),
        query_weight.T,
        key_weight.T,
        value_weight.T,
        gate_weight.T,
        both_cosine,
        both_sine,
        state,
        output_weight,
        group_gain.reshape(1, HEAD_DIM),
    )
    shares, new_state = call(
        retention_kernel,
        (like((kv, served, feats), bf16), like(state.shape, f32)),
        *operands,
        scalars=(decay,),
        hbm=tuple(range(len(operands))),
        out_hbm=(1,),
        scratch=(
            *(pltpu.VMEM(a.shape, a.dtype) for a in operands),
            pltpu.VMEM((served, kv * feats), bf16),
            pltpu.VMEM((served, HEAD_DIM), f32),
            pltpu.VMEM(state.shape, f32),
            pltpu.SemaphoreType.DMA((len(operands),)),
            pltpu.SemaphoreType.DMA((4,)),
        ),
        limit=63 << 20,
        flops=2 * served * D * 6 * HEAD_DIM,
    )
    shares = swap(shares, KV)
    after = call(after_kernel, like((served, feats), bf16), shares, tokens)

    passed = lax.ppermute(after, NEAR, turn)
    copies = call(
        rows_kernel,
        like((cols * cores, 2 * served, feats), bf16),
        after,
        passed,
        scalars=(near,),
    )
    rows = swap(copies, COLS + (CORE,)).reshape(cols, count, feats)
    ups = weights[:, :units]
    own, given = call(
        up_kernel,
        (
            like((count + 8, far * units), f32),
            like((count + 8, far * units), bf16),
        ),
        rows,
        arrived,
        ups,
        flops=2 * count * cols * feats * far * units,
    )
    weights, given = lax.optimization_barrier((weights, given))
    downs = weights[:, units : 2 * units]
    other = lax.ppermute(given, RING, [(0, 3), (1, 2), (2, 1), (3, 0)])
    lowered = call(
        down_kernel,
        like((cols, count, feats), bf16),
        own,
        other,
        downs,
        flops=2 * count * cols * feats * far * units,
    )

    lowered = lowered.reshape(cols * 2 * cores, served, feats)
    lowered = swap(lowered, COLS + (CORE, NEAR))
    mixed = call(final_kernel, like((served, feats), bf16), lowered, after)
    return (mixed, new_state[:, None])


def solution(mesh):
    fine = Mesh(mesh.devices.reshape(4, 2, 2, 2, 2, 2, 2, 2), KV + TP)
    return jax.shard_map(
        layer,
        mesh=fine,
        in_specs=(
            P(TP, KV),
            P(TP),
            P(None, KV),
            P(None, KV),
            P(None, KV),
            P(None, KV),
            P(KV, None),
            P(None),
            P(KV),
            P(KV),
            P(KV, TP),
            P(TP, KV),
            P(TP, KV, None, None),
        ),
        out_specs=(P(TP, KV), P(TP, KV, None, None)),
        check_vma=False,
    )
```

```python
import jax
import jax.numpy as jnp
import numpy as np
from jax import lax
from jax.experimental import pallas as pl
from jax.experimental.pallas import tpu as pltpu
from jax.sharding import Mesh
from jax.sharding import PartitionSpec as P

D = 2048
HEADS = 16
HEAD_DIM = 64
EPS = 1e-06
THETA = 10000.0

KV = ("y", "xh", "xl")
TP = ("b3", "b2", "b1", "b0", "c")
HALF = "xh"
COLS = ("y", "xl")
RING = ("xh", "xl")
NEAR = "b0"
CORE = "c"
FAR = ("b3", "b2", "b1")

bf16, f32 = jnp.bfloat16, jnp.float32
NT = (((1,), (1,)), ((), ()))


def size_of(axes):
    return int(np.prod([lax.axis_size(a) for a in axes]))


def swap(blocks, axes):
    return lax.all_to_all(blocks, axes, split_axis=0, concat_axis=0, tiled=True)


def call(kernel, out, *operands, scalars=(), hbm=(), out_hbm=(), scratch=(), limit=16 << 20, flops=1 << 20):
    outs = out if isinstance(out, tuple) else (out,)
    moved = sum(o.size * o.dtype.itemsize for o in operands)
    moved += sum(int(np.prod(o.shape)) * o.dtype.itemsize for o in outs)
    smem = pl.BlockSpec(memory_space=pltpu.SMEM)
    vmem = pl.BlockSpec(memory_space=pltpu.VMEM)
    far = pl.BlockSpec(memory_space=pltpu.HBM)
    return pl.pallas_call(
        kernel,
        out_shape=out,
        in_specs=[smem] * len(scalars)
        + [far if n in hbm else vmem for n in range(len(operands))],
        out_specs=tuple(far if n in out_hbm else vmem for n in range(len(out)))
        if isinstance(out, tuple)
        else vmem,
        scratch_shapes=scratch,
        compiler_params=pltpu.CompilerParams(vmem_limit_bytes=limit),
        cost_estimate=pl.CostEstimate(flops=flops, bytes_accessed=moved, transcendentals=0),
    )(*(jnp.reshape(v, (1,)) for v in scalars), *operands)


def fetch(pairs, sems):
    copies = [pltpu.make_async_copy(a, b, sems.at[n]) for n, (a, b) in enumerate(pairs)]
    for copy in copies:
        copy.start()
    for copy in copies:
        copy.wait()


def pack_kernel(decay_ref, half_ref, up_hbm, down_hbm, gain_hbm, out_ref, *scratch):
    up_ref, down_ref, gain_ref, sems = scratch
    fetch(
        (
            (up_hbm, up_ref),
            (down_hbm, down_ref),
            (gain_hbm, gain_ref),
        ),
        sems,
    )
    cols = out_ref.shape[0]
    feats, width = up_ref.shape
    units = width // cols
    gain = gain_ref[...]
    first = gain.astype(bf16).astype(f32)
    second = (gain - first).astype(bf16).astype(f32)
    third = gain - first - second
    row = lax.broadcasted_iota(jnp.int32, (8, feats), 0)
    zero = jnp.zeros((8, feats), f32)
    rows = jnp.where(row == 0, first, jnp.where(row == 1, second, jnp.where(row == 2, third, zero)))
    rows = rows.astype(bf16)
    up = up_ref[...].astype(f32).T.astype(bf16)
    down = down_ref[...]
    for j in range(cols):
        at, turned = slice(j * units, (j + 1) * units), slice((j ^ 1) * units, ((j ^ 1) + 1) * units)
        out_ref[j, :units] = jnp.where(half_ref[0] == 0, up[at], up[turned])
        out_ref[j, units : 2 * units] = jnp.where(half_ref[0] == 0, down[at], down[turned])
        out_ref[j, 2 * units :] = rows


def copies_kernel(tokens_ref, copies_ref):
    tokens = tokens_ref[...]
    for k in range(copies_ref.shape[0]):
        copies_ref[k] = tokens


def unpack_kernel(arrived_ref, mine_ref):
    feats = arrived_ref.shape[2]
    both = mine_ref.shape[0]
    for j in range(arrived_ref.shape[0]):
        mine_ref[:, j * feats : (j + 1) * feats] = arrived_ref[j, :both]


def retention_kernel(decay_ref, *refs):
    sources, (shares_ref, new_hbm) = refs[:11], refs[11:13]
    targets, (normed_ref, readout_ref, new_ref, sems, out_sems) = refs[13:24], refs[24:]
    copies = [
        pltpu.make_async_copy(a, b, sems.at[n]) for n, (a, b) in enumerate(zip(sources, targets))
    ]
    for copy in copies:
        copy.start()
    blocks_ref, mixer_ref, query_ref, key_ref, value_ref, gate_ref = targets[:6]
    cosine_ref, sine_ref, state_ref, output_ref, gain_ref = targets[6:]
    kv, served, feats = blocks_ref.shape
    for copy in copies[:2]:
        copy.wait()
    total = jnp.zeros((served, feats), f32)
    for k in range(kv):
        x = blocks_ref[k].astype(f32)
        total = total + x * x
    factor = lax.rsqrt(jnp.sum(total, axis=1, keepdims=True) / D + EPS)
    for k in range(kv):
        at = slice(k * feats, (k + 1) * feats)
        normed_ref[:, at] = (blocks_ref[k].astype(f32) * factor * mixer_ref[:, at]).astype(bf16)
    normed = normed_ref[...]
    middle = HEAD_DIM // 2

    def project(weight):
        return lax.dot_general(normed, weight, NT, preferred_element_type=f32)

    def rotated(ref):
        plain = project(ref[...])
        turned = project(jnp.concatenate([ref[middle:], ref[:middle]]))
        return plain * cosine_ref[...] + turned * sine_ref[...]

    for copy in copies[2:8]:
        copy.wait()
    queries = rotated(query_ref)
    keys = rotated(key_ref) * HEAD_DIM ** (-0.5)
    values = project(value_ref[...])
    gating = project(gate_ref[...])
    columns, key_columns = queries.T, keys.T
    for copy in copies[8:]:
        copy.wait()
    step = served // out_sems.shape[0]
    given = [
        pltpu.make_async_copy(
            new_ref.at[pl.ds(n * step, step)], new_hbm.at[pl.ds(n * step, step)], out_sems.at[n]
        )
        for n in range(out_sems.shape[0])
    ]
    for b in range(served):
        added = key_columns[:, b : b + 1] * values[b : b + 1]
        new_ref[b] = decay_ref[0] * state_ref[b] + added
        if b % step == step - 1 and b > step:
            given[b // step - 1].start()
    for b in range(state_ref.shape[0]):
        readout_ref[b : b + 1] = jnp.sum(state_ref[b] * columns[:, b : b + 1], axis=0, keepdims=True)
    matched = jnp.sum(keys * queries, axis=1, keepdims=True)
    readout = decay_ref[0] * readout_ref[...] + matched * values
    square = jnp.sum(readout * readout, axis=1, keepdims=True) / HEAD_DIM
    grouped = readout * lax.rsqrt(square + EPS) * gain_ref[...]
    merged = (grouped * (gating * jax.nn.sigmoid(gating))).astype(bf16)
    shares = jnp.dot(merged, output_ref[...], preferred_element_type=f32).astype(bf16)
    for k in range(shares_ref.shape[0]):
        shares_ref[k] = shares[:, k * feats : (k + 1) * feats]
    given[-1].start()
    for copy in given:
        copy.wait()


def sum_of(parts_ref):
    total = parts_ref[0].astype(f32)
    for k in range(1, parts_ref.shape[0]):
        total = total + parts_ref[k].astype(f32)
    return total


def after_kernel(parts_ref, tokens_ref, out_ref):
    out_ref[...] = (tokens_ref[...].astype(f32) + sum_of(parts_ref)).astype(bf16)


def rows_kernel(near_ref, own_ref, other_ref, out_ref):
    served = own_ref.shape[0]
    for n in range(2):
        block = jnp.where(near_ref[0] == n, own_ref[...], other_ref[...])
        for p in range(out_ref.shape[0]):
            out_ref[p, n * served : (n + 1) * served] = block


def up_kernel(rows_ref, arrived_ref, weights_ref, own_ref, sent_ref):
    cols, count, feats = rows_ref.shape
    lines = arrived_ref.shape[1]
    far, units, width = weights_ref.shape
    ones = jnp.ones((8, feats), bf16)
    total = jnp.zeros((8, count), f32)
    scaled = []
    for j in range(cols):
        x = rows_ref[j].astype(f32)
        pieces = arrived_ref[j, lines - 8 :].astype(f32)
        scaled.append((x * (pieces[0:1] + pieces[1:2] + pieces[2:3])).astype(bf16))
        square = x * x
        high = square.astype(bf16)
        low = (square - high.astype(f32)).astype(bf16)
        total = total + lax.dot_general(ones, high, NT, preferred_element_type=f32)
        total = total + lax.dot_general(ones, low, NT, preferred_element_type=f32)
    part = lax.dot_general(
        jnp.concatenate(scaled, axis=1),
        weights_ref[...].reshape(far * units, width),
        NT,
        preferred_element_type=f32,
    )
    own_ref[:count] = part
    sent_ref[:count] = part.astype(bf16)
    high = total.astype(bf16).astype(f32)
    low = total - high
    row = lax.broadcasted_iota(jnp.int32, total.shape, 0)
    extra = jnp.where(row == 0, high, jnp.where(row == 1, low, jnp.zeros_like(total)))
    own_ref[count:] = extra
    sent_ref[count:] = extra.astype(bf16)


def down_kernel(own_ref, other_ref, weights_ref, out_ref):
    cols, count, feats = out_ref.shape
    total = own_ref[...] + other_ref[...].astype(f32)
    squares = total[count : count + 1] + total[count + 1 : count + 2]
    row = lax.broadcasted_iota(jnp.int32, (count, count), 0)
    lane = lax.broadcasted_iota(jnp.int32, (count, count), 1)
    mine = jnp.where(lane == row, squares, jnp.zeros((count, count), f32))
    factor = lax.rsqrt(jnp.sum(mine, axis=1, keepdims=True) / D + EPS)
    raised = jnp.maximum(total[:count] * factor, 0.0)
    hidden = (raised * raised).astype(bf16)
    weight = weights_ref[...].reshape(-1, weights_ref.shape[2])
    part = jnp.dot(hidden, weight, preferred_element_type=f32).astype(bf16)
    for j in range(cols):
        out_ref[j] = part[:, j * feats : (j + 1) * feats]


def final_kernel(parts_ref, after_ref, out_ref):
    out_ref[...] = (after_ref[...].astype(f32) + sum_of(parts_ref)).astype(out_ref.dtype)


def layer(
    tokens,
    lengths,
    query_weight,
    key_weight,
    value_weight,
    gate_weight,
    output_weight,
    mixer_gain,
    group_gain,
    channel_gain,
    up_weight,
    down_weight,
    memory_state,
):
    like = jax.ShapeDtypeStruct
    served, feats = tokens.shape
    kv, cols, far = size_of(KV), size_of(COLS), size_of(FAR)
    cores = lax.axis_size(CORE)
    units = up_weight.shape[1] // cols
    count = 2 * cores * served
    near = lax.axis_index(NEAR)
    turn = [(0, 1), (1, 0)]
    head = lax.axis_index(KV).astype(f32)
    decay = 1.0 - 2.0 ** (-5.0 - 5.0 * head / (HEADS - 1))
    sent = call(
        pack_kernel,
        like((cols, 2 * units + 8, feats), bf16),
        up_weight,
        down_weight,
        channel_gain.reshape(1, feats),
        scalars=(decay, lax.axis_index(HALF)),
        hbm=(0, 1, 2),
        limit=63 << 20,
        scratch=(
            pltpu.VMEM(up_weight.shape, bf16),
            pltpu.VMEM(down_weight.shape, bf16),
            pltpu.VMEM((1, feats), f32),
            pltpu.SemaphoreType.DMA((3,)),
        ),
    )
    arrived = swap(sent, COLS)
    mine = call(unpack_kernel, like((2 * units, cols * feats), bf16), arrived)
    weights = lax.all_gather(mine, FAR, axis=0, tiled=True)

    copies = call(copies_kernel, like((kv, served, feats), bf16), tokens)
    blocks = swap(copies, KV)
    middle = HEAD_DIM // 2
    inverse = THETA ** (-jnp.arange(middle, dtype=f32) * 2.0 / HEAD_DIM)
    angles = lengths.astype(f32)[:, None] * inverse[None, :]
    cosine, sine = jnp.cos(angles), jnp.sin(angles)
    both_cosine = jnp.concatenate([cosine, cosine], axis=1)
    both_sine = jnp.concatenate([-sine, sine], axis=1)
    state = memory_state[:, 0]
    operands = (
        blocks,
        mixer_gain.reshape(1, kv * feats),
        query_weight.T,
        key_weight.T,
        value_weight.T,
        gate_weight.T,
        both_cosine,
        both_sine,
        state,
        output_weight,
        group_gain.reshape(1, HEAD_DIM),
    )
    shares, new_state = call(
        retention_kernel,
        (like((kv, served, feats), bf16), like(state.shape, f32)),
        *operands,
        scalars=(decay,),
        hbm=tuple(range(len(operands))),
        out_hbm=(1,),
        scratch=(
            *(pltpu.VMEM(a.shape, a.dtype) for a in operands),
            pltpu.VMEM((served, kv * feats), bf16),
            pltpu.VMEM((served, HEAD_DIM), f32),
            pltpu.VMEM(state.shape, f32),
            pltpu.SemaphoreType.DMA((len(operands),)),
            pltpu.SemaphoreType.DMA((4,)),
        ),
        limit=63 << 20,
        flops=2 * served * D * 6 * HEAD_DIM,
    )
    shares = swap(shares, KV)
    after = call(after_kernel, like((served, feats), bf16), shares, tokens)

    passed = lax.ppermute(after, NEAR, turn)
    copies = call(
        rows_kernel,
        like((cols * cores, 2 * served, feats), bf16),
        after,
        passed,
        scalars=(near,),
    )
    rows = swap(copies, COLS + (CORE,)).reshape(cols, count, feats)
    weights = weights.reshape(far, 2, units, cols * feats)
    ups = weights[:, 0]
    own, given = call(
        up_kernel,
        (
            like((count + 8, far * units), f32),
            like((count + 8, far * units), bf16),
        ),
        rows,
        arrived,
        ups,
        flops=2 * count * cols * feats * far * units,
    )
    weights, given = lax.optimization_barrier((weights, given))
    downs = weights[:, 1]
    other = lax.ppermute(given, RING, [(0, 3), (1, 2), (2, 1), (3, 0)])
    lowered = call(
        down_kernel,
        like((cols, count, feats), bf16),
        own,
        other,
        downs,
        flops=2 * count * cols * feats * far * units,
    )

    lowered = lowered.reshape(cols * 2 * cores, served, feats)
    lowered = swap(lowered, COLS + (CORE, NEAR))
    mixed = call(final_kernel, like((served, feats), bf16), lowered, after)
    return (mixed, new_state[:, None])


def solution(mesh):
    fine = Mesh(mesh.devices.reshape(4, 2, 2, 2, 2, 2, 2, 2), KV + TP)
    return jax.shard_map(
        layer,
        mesh=fine,
        in_specs=(
            P(TP, KV),
            P(TP),
            P(None, KV),
            P(None, KV),
            P(None, KV),
            P(None, KV),
            P(KV, None),
            P(None),
            P(KV),
            P(KV),
            P(KV, TP),
            P(TP, KV),
            P(TP, KV, None, None),
        ),
        out_specs=(P(TP, KV), P(TP, KV, None, None)),
        check_vma=False,
    )
```

```python
import jax
import jax.numpy as jnp
import numpy as np
from jax import lax
from jax.experimental import pallas as pl
from jax.experimental.pallas import tpu as pltpu
from jax.sharding import Mesh
from jax.sharding import PartitionSpec as P

D = 2048
HEADS = 16
HEAD_DIM = 64
EPS = 1e-06
THETA = 10000.0

KV = ("y", "xh", "xl")
TP = ("b3", "b2", "b1", "b0", "c")
HALF = "xh"
COLS = ("y", "xl")
RING = ("xh", "xl")
NEAR = "b0"
CORE = "c"
FAR = ("b3", "b2", "b1")

bf16, f32 = jnp.bfloat16, jnp.float32
NT = (((1,), (1,)), ((), ()))


def size_of(axes):
    return int(np.prod([lax.axis_size(a) for a in axes]))


def swap(blocks, axes):
    return lax.all_to_all(blocks, axes, split_axis=0, concat_axis=0, tiled=True)


def call(kernel, out, *operands, scalars=(), hbm=(), out_hbm=(), scratch=(), limit=16 << 20, flops=1 << 20):
    outs = out if isinstance(out, tuple) else (out,)
    moved = sum(o.size * o.dtype.itemsize for o in operands)
    moved += sum(int(np.prod(o.shape)) * o.dtype.itemsize for o in outs)
    smem = pl.BlockSpec(memory_space=pltpu.SMEM)
    vmem = pl.BlockSpec(memory_space=pltpu.VMEM)
    far = pl.BlockSpec(memory_space=pltpu.HBM)
    return pl.pallas_call(
        kernel,
        out_shape=out,
        in_specs=[smem] * len(scalars)
        + [far if n in hbm else vmem for n in range(len(operands))],
        out_specs=tuple(far if n in out_hbm else vmem for n in range(len(out)))
        if isinstance(out, tuple)
        else vmem,
        scratch_shapes=scratch,
        compiler_params=pltpu.CompilerParams(vmem_limit_bytes=limit),
        cost_estimate=pl.CostEstimate(flops=flops, bytes_accessed=moved, transcendentals=0),
    )(*(jnp.reshape(v, (1,)) for v in scalars), *operands)


def fetch(pairs, sems):
    copies = [pltpu.make_async_copy(a, b, sems.at[n]) for n, (a, b) in enumerate(pairs)]
    for copy in copies:
        copy.start()
    for copy in copies:
        copy.wait()


def pack_kernel(decay_ref, half_ref, up_hbm, down_hbm, gain_hbm, out_ref, *scratch):
    up_ref, down_ref, gain_ref, sems = scratch
    fetch(
        (
            (up_hbm, up_ref),
            (down_hbm, down_ref),
            (gain_hbm, gain_ref),
        ),
        sems,
    )
    cols = out_ref.shape[0]
    feats, width = up_ref.shape
    units = width // cols
    gain = gain_ref[...]
    first = gain.astype(bf16).astype(f32)
    second = (gain - first).astype(bf16).astype(f32)
    third = gain - first - second
    row = lax.broadcasted_iota(jnp.int32, (8, feats), 0)
    zero = jnp.zeros((8, feats), f32)
    rows = jnp.where(row == 0, first, jnp.where(row == 1, second, jnp.where(row == 2, third, zero)))
    rows = rows.astype(bf16)
    up = up_ref[...].astype(f32).T.astype(bf16)
    down = down_ref[...]
    for j in range(cols):
        at, turned = slice(j * units, (j + 1) * units), slice((j ^ 1) * units, ((j ^ 1) + 1) * units)
        out_ref[j, :units] = jnp.where(half_ref[0] == 0, up[at], up[turned])
        out_ref[j, units : 2 * units] = jnp.where(half_ref[0] == 0, down[at], down[turned])
        out_ref[j, 2 * units :] = rows


def copies_kernel(tokens_ref, copies_ref):
    tokens = tokens_ref[...]
    for k in range(copies_ref.shape[0]):
        copies_ref[k] = tokens


def unpack_kernel(arrived_ref, mine_ref):
    feats = arrived_ref.shape[2]
    both = mine_ref.shape[0]
    for j in range(arrived_ref.shape[0]):
        mine_ref[:, j * feats : (j + 1) * feats] = arrived_ref[j, :both]


def retention_kernel(decay_ref, *refs):
    sources, (shares_ref, keys_ref, values_ref) = refs[:11], refs[11:14]
    targets, (normed_ref, readout_ref, sems) = refs[14:25], refs[25:]
    copies = [
        pltpu.make_async_copy(a, b, sems.at[n]) for n, (a, b) in enumerate(zip(sources, targets))
    ]
    for copy in copies:
        copy.start()
    blocks_ref, mixer_ref, query_ref, key_ref, value_ref, gate_ref = targets[:6]
    cosine_ref, sine_ref, state_ref, output_ref, gain_ref = targets[6:]
    kv, served, feats = blocks_ref.shape
    for copy in copies[:2]:
        copy.wait()
    total = jnp.zeros((served, feats), f32)
    for k in range(kv):
        x = blocks_ref[k].astype(f32)
        total = total + x * x
    factor = lax.rsqrt(jnp.sum(total, axis=1, keepdims=True) / D + EPS)
    for k in range(kv):
        at = slice(k * feats, (k + 1) * feats)
        normed_ref[:, at] = (blocks_ref[k].astype(f32) * factor * mixer_ref[:, at]).astype(bf16)
    normed = normed_ref[...]
    middle = HEAD_DIM // 2

    def project(weight):
        return lax.dot_general(normed, weight, NT, preferred_element_type=f32)

    def rotated(ref):
        plain = project(ref[...])
        turned = project(jnp.concatenate([ref[middle:], ref[:middle]]))
        return plain * cosine_ref[...] + turned * sine_ref[...]

    for copy in copies[2:8]:
        copy.wait()
    queries = rotated(query_ref)
    keys = rotated(key_ref) * HEAD_DIM ** (-0.5)
    values = project(value_ref[...])
    gating = project(gate_ref[...])
    keys_ref[...] = keys
    values_ref[...] = values
    columns = queries.T
    for copy in copies[8:]:
        copy.wait()
    for b in range(state_ref.shape[0]):
        readout_ref[b : b + 1] = jnp.sum(state_ref[b] * columns[:, b : b + 1], axis=0, keepdims=True)
    matched = jnp.sum(keys * queries, axis=1, keepdims=True)
    readout = decay_ref[0] * readout_ref[...] + matched * values
    square = jnp.sum(readout * readout, axis=1, keepdims=True) / HEAD_DIM
    grouped = readout * lax.rsqrt(square + EPS) * gain_ref[...]
    merged = (grouped * (gating * jax.nn.sigmoid(gating))).astype(bf16)
    shares = jnp.dot(merged, output_ref[...], preferred_element_type=f32).astype(bf16)
    feats = shares_ref.shape[2]
    for k in range(shares_ref.shape[0]):
        shares_ref[k] = shares[:, k * feats : (k + 1) * feats]


def sum_of(parts_ref):
    total = parts_ref[0].astype(f32)
    for k in range(1, parts_ref.shape[0]):
        total = total + parts_ref[k].astype(f32)
    return total


def after_kernel(parts_ref, tokens_ref, out_ref):
    out_ref[...] = (tokens_ref[...].astype(f32) + sum_of(parts_ref)).astype(bf16)


def rows_kernel(near_ref, own_ref, other_ref, out_ref):
    served = own_ref.shape[0]
    for n in range(2):
        block = jnp.where(near_ref[0] == n, own_ref[...], other_ref[...])
        for p in range(out_ref.shape[0]):
            out_ref[p, n * served : (n + 1) * served] = block


def up_kernel(rows_ref, arrived_ref, weights_ref, own_ref, sent_ref):
    cols, count, feats = rows_ref.shape
    lines = arrived_ref.shape[1]
    far, units, width = weights_ref.shape
    ones = jnp.ones((8, feats), bf16)
    total = jnp.zeros((8, count), f32)
    scaled = []
    for j in range(cols):
        x = rows_ref[j].astype(f32)
        pieces = arrived_ref[j, lines - 8 :].astype(f32)
        scaled.append((x * (pieces[0:1] + pieces[1:2] + pieces[2:3])).astype(bf16))
        square = x * x
        high = square.astype(bf16)
        low = (square - high.astype(f32)).astype(bf16)
        total = total + lax.dot_general(ones, high, NT, preferred_element_type=f32)
        total = total + lax.dot_general(ones, low, NT, preferred_element_type=f32)
    part = lax.dot_general(
        jnp.concatenate(scaled, axis=1),
        weights_ref[...].reshape(far * units, width),
        NT,
        preferred_element_type=f32,
    )
    own_ref[:count] = part
    sent_ref[:count] = part.astype(bf16)
    high = total.astype(bf16).astype(f32)
    low = total - high
    row = lax.broadcasted_iota(jnp.int32, total.shape, 0)
    extra = jnp.where(row == 0, high, jnp.where(row == 1, low, jnp.zeros_like(total)))
    own_ref[count:] = extra
    sent_ref[count:] = extra.astype(bf16)


def down_kernel(own_ref, other_ref, weights_ref, out_ref):
    cols, count, feats = out_ref.shape
    total = own_ref[...] + other_ref[...].astype(f32)
    squares = total[count : count + 1] + total[count + 1 : count + 2]
    row = lax.broadcasted_iota(jnp.int32, (count, count), 0)
    lane = lax.broadcasted_iota(jnp.int32, (count, count), 1)
    mine = jnp.where(lane == row, squares, jnp.zeros((count, count), f32))
    factor = lax.rsqrt(jnp.sum(mine, axis=1, keepdims=True) / D + EPS)
    raised = jnp.maximum(total[:count] * factor, 0.0)
    hidden = (raised * raised).astype(bf16)
    weight = weights_ref[...].reshape(-1, weights_ref.shape[2])
    part = jnp.dot(hidden, weight, preferred_element_type=f32).astype(bf16)
    for j in range(cols):
        out_ref[j] = part[:, j * feats : (j + 1) * feats]


def final_kernel(parts_ref, after_ref, out_ref):
    out_ref[...] = (after_ref[...].astype(f32) + sum_of(parts_ref)).astype(out_ref.dtype)


def layer(
    tokens,
    lengths,
    query_weight,
    key_weight,
    value_weight,
    gate_weight,
    output_weight,
    mixer_gain,
    group_gain,
    channel_gain,
    up_weight,
    down_weight,
    memory_state,
):
    like = jax.ShapeDtypeStruct
    served, feats = tokens.shape
    kv, cols, far = size_of(KV), size_of(COLS), size_of(FAR)
    cores = lax.axis_size(CORE)
    units = up_weight.shape[1] // cols
    count = 2 * cores * served
    near = lax.axis_index(NEAR)
    turn = [(0, 1), (1, 0)]
    head = lax.axis_index(KV).astype(f32)
    decay = 1.0 - 2.0 ** (-5.0 - 5.0 * head / (HEADS - 1))
    sent = call(
        pack_kernel,
        like((cols, 2 * units + 8, feats), bf16),
        up_weight,
        down_weight,
        channel_gain.reshape(1, feats),
        scalars=(decay, lax.axis_index(HALF)),
        hbm=(0, 1, 2),
        limit=63 << 20,
        scratch=(
            pltpu.VMEM(up_weight.shape, bf16),
            pltpu.VMEM(down_weight.shape, bf16),
            pltpu.VMEM((1, feats), f32),
            pltpu.SemaphoreType.DMA((3,)),
        ),
    )
    arrived = swap(sent, COLS)
    mine = call(unpack_kernel, like((2 * units, cols * feats), bf16), arrived)
    weights = lax.all_gather(mine, FAR, axis=0, tiled=True)

    copies = call(copies_kernel, like((kv, served, feats), bf16), tokens)
    blocks = swap(copies, KV)
    middle = HEAD_DIM // 2
    inverse = THETA ** (-jnp.arange(middle, dtype=f32) * 2.0 / HEAD_DIM)
    angles = lengths.astype(f32)[:, None] * inverse[None, :]
    cosine, sine = jnp.cos(angles), jnp.sin(angles)
    both_cosine = jnp.concatenate([cosine, cosine], axis=1)
    both_sine = jnp.concatenate([-sine, sine], axis=1)
    state = memory_state[:, 0]
    operands = (
        blocks,
        mixer_gain.reshape(1, kv * feats),
        query_weight.T,
        key_weight.T,
        value_weight.T,
        gate_weight.T,
        both_cosine,
        both_sine,
        state,
        output_weight,
        group_gain.reshape(1, HEAD_DIM),
    )
    shares, keys_new, values_new = call(
        retention_kernel,
        (
            like((kv, served, feats), bf16),
            like((served, HEAD_DIM), f32),
            like((served, HEAD_DIM), f32),
        ),
        *operands,
        scalars=(decay,),
        hbm=tuple(range(len(operands))),
        scratch=(
            *(pltpu.VMEM(a.shape, a.dtype) for a in operands),
            pltpu.VMEM((served, kv * feats), bf16),
            pltpu.VMEM((served, HEAD_DIM), f32),
            pltpu.SemaphoreType.DMA((len(operands),)),
        ),
        limit=63 << 20,
        flops=2 * served * D * 6 * HEAD_DIM,
    )
    shares = swap(shares, KV)
    after = call(after_kernel, like((served, feats), bf16), shares, tokens)

    passed = lax.ppermute(after, NEAR, turn)
    copies = call(
        rows_kernel,
        like((cols * cores, 2 * served, feats), bf16),
        after,
        passed,
        scalars=(near,),
    )
    rows = swap(copies, COLS + (CORE,)).reshape(cols, count, feats)
    weights = weights.reshape(far, 2, units, cols * feats)
    ups = weights[:, 0]
    own, given = call(
        up_kernel,
        (
            like((count + 8, far * units), f32),
            like((count + 8, far * units), bf16),
        ),
        rows,
        arrived,
        ups,
        flops=2 * count * cols * feats * far * units,
    )
    weights, given = lax.optimization_barrier((weights, given))
    downs = weights[:, 1]
    other = lax.ppermute(given, RING, [(0, 3), (1, 2), (2, 1), (3, 0)])
    lowered = call(
        down_kernel,
        like((cols, count, feats), bf16),
        own,
        other,
        downs,
        flops=2 * count * cols * feats * far * units,
    )

    lowered = lowered.reshape(cols * 2 * cores, served, feats)
    lowered = swap(lowered, COLS + (CORE, NEAR))
    mixed = call(final_kernel, like((served, feats), bf16), lowered, after)
    new_state = decay * state + keys_new[:, :, None] * values_new[:, None, :]
    return (mixed, new_state[:, None])


def solution(mesh):
    fine = Mesh(mesh.devices.reshape(4, 2, 2, 2, 2, 2, 2, 2), KV + TP)
    return jax.shard_map(
        layer,
        mesh=fine,
        in_specs=(
            P(TP, KV),
            P(TP),
            P(None, KV),
            P(None, KV),
            P(None, KV),
            P(None, KV),
            P(KV, None),
            P(None),
            P(KV),
            P(KV),
            P(KV, TP),
            P(TP, KV),
            P(TP, KV, None, None),
        ),
        out_specs=(P(TP, KV), P(TP, KV, None, None)),
        check_vma=False,
    )
```
